32 devices in a mesh: dp: 4 (over y, x), kv: 4 (over z), tp: 2 (over core).
Axes of the slice: x: 2, y: 2, z: 4, core: 2. Of those that a mesh axis runs over, the one named last changes fastest.
Arguments:
- tokens: bfloat16 [64, 2048], P('dp', ('kv', 'tp')), may hold values from -30 to 30
- state: float32 [64, 4, 256, 512], P(('dp', 'kv'), 'tp'), may hold values from -6 to 6
- mix_gain: float32 [2048], P('kv'), may hold values from 0.1 to 1.9
- w_query: bfloat16 [2048, 1024], P('kv', 'tp'), may hold values from -0.125 to 0.125
- w_key: bfloat16 [2048, 1024], P('kv', 'tp'), may hold values from -0.125 to 0.125
- w_decay: bfloat16 [2048, 1024], P('kv', 'tp'), may hold values from -0.125 to 0.125
- w_value: bfloat16 [2048, 2048], P('kv', 'tp'), may hold values from -0.125 to 0.125
- w_gate: bfloat16 [2048, 2048], P('kv', 'tp'), may hold values from -0.125 to 0.125
- decay_offset: float32 [1024], P('tp'), may hold values from -1 to 4
- head_gain: float32 [512], replicated, may hold values from 0.1 to 1.9
- w_out: bfloat16 [2048, 2048], P('tp', 'kv'), may hold values from -0.125 to 0.125
- mlp_gain: float32 [2048], replicated, may hold values from 0.1 to 1.9
- w_up: bfloat16 [2048, 8192], P(None, ('kv', 'tp')), may hold values from -0.125 to 0.125
- w_down: bfloat16 [8192, 2048], P(('kv', 'tp')), may hold values from -0.09375 to 0.09375
Outputs:
- mixed: bfloat16 [64, 2048], P('dp', ('kv', 'tp'))
- new_state: float32 [64, 4, 256, 512], P(('dp', 'kv'), 'tp')
The draws below stay inside these ranges and needn't reach their ends.
All inputs are finite; a program needn't handle non-finite values.
Results may differ from the reference program's by a relative error of at most 0.013.
Values may be sent and summed in bfloat16 or wider, within the bound.
A program may use at most 64 MiB of HBM per device.

```python
import math
import jax
import jax.numpy as jnp
from jax import lax

D = 2048
HEADS = 4
KEY_DIM = 256
VAL_DIM = 512
FF = 8192
BATCH = 64


def draw_tokens(key, part):
    base_key, row_key = jax.random.split(key)
    columns = jnp.exp(jnp.linspace(math.log(0.4), math.log(2.4), D)).astype(jnp.float32)
    base = jnp.clip(jax.random.normal(base_key, (BATCH, D), jnp.float32), -6.0, 6.0)
    rowwise = jnp.exp(jax.random.uniform(row_key, (BATCH,), jnp.float32, math.log(0.5), math.log(2.0)))
    return (base * rowwise[:, None] * columns[None, :]).astype(jnp.bfloat16)


def strengthened(entries, key, source, target, blocks, factor):
    owner, partner = [(jnp.arange(entries.shape[dim]) // (entries.shape[dim] // blocks)).reshape([-1 if axis == dim else 1 for axis in range(entries.ndim)]) for dim in (source, target)]
    chosen = jax.random.permutation(key, blocks)[partner]
    strong = (owner == chosen) | (owner == (partner + blocks // 2) % blocks)
    return jnp.where(strong, factor * entries, entries)


def shard_levels(key, shape, shards, smallest, largest):
    factor_of = 1.0
    for axis_at, parts in shards:
        heights = jax.random.uniform(jax.random.fold_in(jax.random.fold_in(key, 6), axis_at), (parts,), jnp.float32, smallest / len(shards), largest / len(shards))
        factor_of = factor_of * jnp.repeat(jnp.exp(heights), shape[axis_at] // parts).reshape((-1,) + (1,) * (len(shape) - 1 - axis_at))
    return factor_of


def centred(stream_key, dims, scale, most, shards=(), kind=jnp.bfloat16):
    array = jax.random.normal(stream_key, dims, jnp.float32) * scale
    if len(shards) > 0:
        array = shard_levels(stream_key, dims, shards, -0.22, 0.18) * array
    return jnp.clip(array, min=-most, max=most).astype(kind)


def heavy_noise(rng, extent, scale, limit, cuts, heavy, held_as=jnp.bfloat16):
    entries = scale * jax.random.normal(rng, extent, jnp.float32)
    if cuts:
        entries = entries * shard_levels(rng, extent, cuts, -0.22, 0.18)
    return jnp.clip(strengthened(entries, jax.random.fold_in(rng, 3), *heavy), -limit, limit).astype(held_as)


def setup_inputs(seed: int = 0) -> dict:
    key_list = jax.random.split(jax.random.key(seed), 15)
    return {
        "tokens": draw_tokens(jax.random.fold_in(key_list[14], 71), 0),
        "state": centred(key_list[1], (BATCH, HEADS, KEY_DIM, VAL_DIM), 1.0, 6.0, ((0, 16), (1, 2)), jnp.float32),
        "mix_gain": jnp.clip(1.0 + 0.18 * jax.random.normal(key_list[2], (D,), jnp.float32), 0.1, 1.9),
        "w_query": centred(key_list[3], (D, HEADS * KEY_DIM), D ** -0.5, 0.125, ((0, 4), (1, 2))),
        "w_key": centred(key_list[4], (D, HEADS * KEY_DIM), D ** -0.5, 0.125, ((0, 4), (1, 2))),
        "w_decay": centred(key_list[5], (D, HEADS * KEY_DIM), D ** -0.5, 0.125, ((0, 4), (1, 2))),
        "w_value": centred(key_list[6], (D, HEADS * VAL_DIM), D ** -0.5, 0.125, ((0, 4), (1, 2))),
        "w_gate": centred(key_list[7], (D, HEADS * VAL_DIM), D ** -0.5, 0.125, ((0, 4), (1, 2))),
        "decay_offset": jnp.clip(-1.0 + 5.0 * jax.random.uniform(key_list[8], (HEADS * KEY_DIM,), jnp.float32) ** shard_levels(key_list[8], (HEADS * KEY_DIM,), ((0, 2),), -0.2, 0.2), -1.0, 4.0),
        "head_gain": jnp.clip(1.0 + 0.18 * jax.random.normal(key_list[9], (VAL_DIM,), jnp.float32), 0.1, 1.9),
        "w_out": centred(key_list[10], (HEADS * VAL_DIM, D), (HEADS * VAL_DIM) ** -0.5, 0.125, ((0, 2), (1, 4))),
        "mlp_gain": jnp.clip(1.0 + 0.18 * jax.random.normal(key_list[11], (D,), jnp.float32), 0.1, 1.9),
        "w_up": centred(key_list[12], (D, FF), D ** -0.5, 0.125, ((1, 8),)),
        "w_down": heavy_noise(key_list[13], (FF, D), FF ** -0.5, 0.09375, ((0, 8),), (0, 1, 8, 2.0)),
    }


epsilon = 1e-06

def reference(tokens, state, mix_gain, w_query, w_key, w_decay, w_value, w_gate, decay_offset, head_gain, w_out, mlp_gain, w_up, w_down):
    tok_float = tokens.astype(jnp.float32)
    row_scale = lax.rsqrt(lax.optimization_barrier(jnp.mean(tok_float * tok_float, axis=1, keepdims=True)) + epsilon)
    scaled = (tok_float * mix_gain).astype(jnp.bfloat16)

    def project(weight):
        return jnp.dot(scaled, weight, preferred_element_type=jnp.float32) * row_scale
    queries = (project(w_query) * KEY_DIM ** (-0.5)).reshape(BATCH, HEADS, KEY_DIM)
    new_keys = project(w_key).reshape(BATCH, HEADS, KEY_DIM)
    values = project(w_value).reshape(BATCH, HEADS, VAL_DIM)
    gates = project(w_gate)
    retain = jax.nn.sigmoid(project(w_decay) + decay_offset).reshape(BATCH, HEADS, KEY_DIM)
    new_state = retain[..., None] * state + new_keys[..., None] * values[:, :, None, :]
    readout = jnp.einsum('bhk,bhkv->bhv', queries, new_state, precision=lax.Precision.HIGHEST)
    readout = readout * lax.rsqrt(lax.optimization_barrier(jnp.mean(readout * readout, axis=2, keepdims=True)) + epsilon) * head_gain
    gated = (readout.reshape(BATCH, HEADS * VAL_DIM) * jax.nn.silu(gates)).astype(jnp.bfloat16)
    stream = (tok_float + jnp.dot(gated, w_out, preferred_element_type=jnp.float32)).astype(jnp.bfloat16)
    stream_float = stream.astype(jnp.float32)
    mlp_scale = lax.rsqrt(lax.optimization_barrier(jnp.mean(stream_float * stream_float, axis=1, keepdims=True)) + epsilon)
    normed = (stream_float * mlp_gain).astype(jnp.bfloat16)
    hidden = jnp.dot(normed, w_up, preferred_element_type=jnp.float32) * mlp_scale
    squared = jnp.square(jax.nn.relu(hidden)).astype(jnp.bfloat16)
    mixed = (stream_float + jnp.dot(squared, w_down, preferred_element_type=jnp.float32)).astype(jnp.bfloat16)
    return (mixed, new_state)
```

```python
import functools

import jax
import jax.numpy as jnp
from jax import lax
from jax.experimental import pallas as pl
from jax.experimental.pallas import tpu as pltpu
from jax.sharding import PartitionSpec as P

D = 2048


epsilon = 1e-06


def plain_shards(
    tokens,
    state,
    mix_gain,
    w_query,
    w_key,
    w_decay,
    w_value,
    w_gate,
    decay_offset,
    head_gain,
    w_out,
    mlp_gain,
    w_up,
    w_down,
):
    seq_dev = state.shape[0]
    heads_here = state.shape[1]
    key_dim = state.shape[2]
    val_dim = state.shape[3]
    weights = (w_query, w_key, w_decay, w_value, w_gate)
    tok_cols = lax.all_gather(tokens, "tp", axis=1, tiled=True)
    tok_float = tok_cols.astype(jnp.float32)
    squares = jnp.sum(tok_float * tok_float, axis=1)
    scaled = (tok_float * mix_gain).astype(jnp.bfloat16)
    kv_index = lax.axis_index("kv")
    projected = lax.psum_scatter(
        jnp.concatenate(
            [jnp.dot(scaled, weight, preferred_element_type=jnp.float32) for weight in weights],
            axis=1,
        ),
        "kv",
        scatter_dimension=0,
        tiled=True,
    )
    all_sums = lax.psum(squares, "kv")
    row_sums = lax.dynamic_slice_in_dim(all_sums, kv_index * seq_dev, seq_dev, 0)
    row_scale = lax.rsqrt(row_sums / D + epsilon)[:, None]
    projected = projected * row_scale
    key_width = heads_here * key_dim
    val_width = heads_here * val_dim
    queries = (projected[:, :key_width] * key_dim ** (-0.5)).reshape(seq_dev, heads_here, key_dim)
    new_keys = projected[:, key_width : 2 * key_width].reshape(seq_dev, heads_here, key_dim)
    retain = jax.nn.sigmoid(projected[:, 2 * key_width : 3 * key_width] + decay_offset).reshape(
        seq_dev, heads_here, key_dim
    )
    values = projected[:, 3 * key_width : 3 * key_width + val_width].reshape(
        seq_dev, heads_here, val_dim
    )
    gates = projected[:, 3 * key_width + val_width :]
    new_state = retain[..., None] * state + new_keys[..., None] * values[:, :, None, :]
    readout = jnp.einsum("bhk,bhkv->bhv", queries, new_state, precision=lax.Precision.HIGHEST)
    readout = (
        readout
        * lax.rsqrt(jnp.mean(readout * readout, axis=2, keepdims=True) + epsilon)
        * head_gain
    )
    gated = (readout.reshape(seq_dev, val_width) * jax.nn.silu(gates)).astype(jnp.bfloat16)
    branch = jnp.dot(
        lax.all_gather(gated, "kv", axis=0, tiled=True), w_out, preferred_element_type=jnp.float32
    )
    own_width = tokens.shape[1]
    branch_total = lax.psum(branch.astype(jnp.bfloat16), "tp").astype(jnp.float32)
    stream_cols = (tok_float + branch_total).astype(jnp.bfloat16)
    stream = lax.all_gather(stream_cols, "kv", axis=1, tiled=True)
    stream_own = lax.dynamic_slice_in_dim(
        stream_cols, lax.axis_index("tp") * own_width, own_width, 1
    )
    stream_float = stream.astype(jnp.float32)
    mlp_scale = lax.rsqrt(jnp.mean(stream_float * stream_float, axis=1, keepdims=True) + epsilon)
    normed = (stream_float * mlp_gain).astype(jnp.bfloat16)
    hidden = jnp.dot(normed, w_up, preferred_element_type=jnp.float32) * mlp_scale
    squared = jnp.square(jax.nn.relu(hidden)).astype(jnp.bfloat16)
    down_own = lax.psum_scatter(
        lax.dot_general(
            w_down, squared, (((0,), (1,)), ((), ())), preferred_element_type=jnp.float32
        ),
        ("kv", "tp"),
        scatter_dimension=0,
        tiled=True,
    )
    mixed = (stream_own.astype(jnp.float32) + down_own.T).astype(jnp.bfloat16)
    return (mixed, new_state)


MESH = pl.DeviceIdType.MESH
ROW_CHUNK = 64
VMEM_BYTES = 67_043_328


def pick(index, values):
    chosen = values[0]
    for at in range(1, len(values)):
        chosen = jnp.where(index == at, values[at], chosen)
    return chosen


def far_first(n_kv, kv):
    orders = [
        sorted((j for j in range(n_kv) if j != me), key=lambda j: (-abs(j - me), j)) for me in range(n_kv)
    ]
    return [pick(kv, [order[at] for order in orders]) for at in range(n_kv - 1)]


def layer_kernel(
    n_kv,
    tok_hbm,
    mix_gain_hbm,
    decay_offset_hbm,
    head_gain_hbm,
    mlp_gain_hbm,
    state_hbm,
    wq_hbm,
    wk_hbm,
    wd_hbm,
    wv_hbm,
    wg_hbm,
    w_out_hbm,
    w_up_hbm,
    w_down_hbm,
    mixed_ref,
    state_ref,
    tok_ref,
    mix_gain_ref,
    decay_offset_ref,
    head_gain_ref,
    mlp_gain_ref,
    wq_ref,
    wk_ref,
    wd_ref,
    wv_ref,
    wg_ref,
    w_out_ref,
    w_up_ref,
    w_down_ref,
    w_out_other,
    tok_all,
    send_a,
    send_b,
    send_c,
    recv_a,
    recv_b,
    recv_c,
    coef,
    coef_t,
    vals,
    read,
    gated_all,
    gated_rows,
    stream_all,
    down_send,
    down_own,
    down_recv,
    load_sem,
    pair_sem,
    go_sem,
    tok_sem,
    w_out_sem,
    proj_send_sem,
    proj_recv_sem,
    gated_send_sem,
    gated_recv_sem,
    stream_send_sem,
    stream_recv_sem,
    down_send_sem,
    down_recv_sem,
):
    f32, bf16 = jnp.float32, jnp.bfloat16
    kv, tp = lax.axis_index("kv"), lax.axis_index("tp")
    other = 1 - tp
    rows, half = tok_ref.shape
    seqs, heads, key_dim, val_dim = state_ref.shape
    key_width, val_width = heads * key_dim, heads * val_dim
    width = 2 * n_kv * half
    far = far_first(n_kv, kv)
    near = far[::-1]

    def remote(src, dst, send_sem, recv_sem, to_kv, to_tp):
        return pltpu.make_async_remote_copy(
            src_ref=src,
            dst_ref=dst,
            send_sem=send_sem,
            recv_sem=recv_sem,
            device_id={"kv": to_kv, "tp": to_tp},
            device_id_type=MESH,
        )

    def signal(sem, to_kv, to_tp):
        pl.semaphore_signal(sem, inc=1, device_id={"kv": to_kv, "tp": to_tp}, device_id_type=MESH)

    barrier = pltpu.get_barrier_semaphore()

    @pl.when(tp == 1)
    def _():
        signal(barrier, kv, 0)

    for j in far:
        signal(barrier, j, 1)

    loads = {}
    for at, (name, source, target) in enumerate(
        (
            ("tokens", tok_hbm, tok_ref),
            ("mix_gain", mix_gain_hbm, mix_gain_ref),
            ("q", wq_hbm, wq_ref),
            ("k", wk_hbm, wk_ref),
            ("d", wd_hbm, wd_ref),
            ("v", wv_hbm, wv_ref),
            ("g", wg_hbm, wg_ref),
            ("offset", decay_offset_hbm, decay_offset_ref),
            ("head_gain", head_gain_hbm, head_gain_ref),
            ("mlp_gain", mlp_gain_hbm, mlp_gain_ref),
            ("state", state_hbm, state_ref),
            ("up", w_up_hbm, w_up_ref),
            ("down", w_down_hbm, w_down_ref),
            ("out", w_out_hbm, w_out_ref),
        )
    ):
        loads[name] = pltpu.make_async_copy(source, target, load_sem.at[at])
        if name != "out":
            loads[name].start()

    @pl.when(tp == 0)
    def _():
        pl.semaphore_wait(barrier, 1)
        signal(pair_sem, kv, 1)

    @pl.when(tp == 1)
    def _():
        loads["out"].start()
        pl.semaphore_wait(pair_sem, 1)

    loads["tokens"].wait()
    tok_copy = remote(tok_ref, tok_all.at[tp], tok_sem.at[0], tok_sem.at[1], kv, other)
    tok_copy.start()
    tok_all[tp] = tok_ref[...]
    tok_own = tok_ref[...].astype(f32)
    squares = jnp.sum(tok_own * tok_own, axis=1, keepdims=True)
    for name in ("mix_gain", "offset", "head_gain", "mlp_gain"):
        loads[name].wait()
    tok_copy.wait_recv()

    @pl.when(tp == 1)
    def _():
        pl.semaphore_wait(barrier, 2 * (n_kv - 1))
        signal(go_sem, kv, 0)

    tok_other = tok_all[other].astype(f32)
    squares = squares + jnp.sum(tok_other * tok_other, axis=1, keepdims=True)
    scaled = jnp.concatenate(
        [(tok_all[i].astype(f32) * mix_gain_ref[i]).astype(bf16) for i in range(2)], axis=1
    )

    def project(name, weight_ref, send, at):
        loads[name].wait()
        total = jnp.dot(scaled, weight_ref[...], preferred_element_type=f32)
        columns = total.shape[1]
        for owner in range(n_kv):
            send[owner, :, at : at + columns] = total[owner * seqs : (owner + 1) * seqs].astype(bf16)

    groups = ((send_a, recv_a), (send_b, recv_b), (send_c, recv_c))

    def proj_copy(group, j, slot):
        send, recv = groups[group]
        return remote(
            send.at[j], recv.at[slot], proj_send_sem.at[group, j], proj_recv_sem.at[group, slot], j, tp
        )

    def send_group(group):
        for j in far:
            proj_copy(group, j, kv).start()

    wide = jnp.broadcast_to(squares, (rows, 128))
    lane = lax.broadcasted_iota(jnp.int32, (seqs, 128), 1)
    for owner in range(n_kv):
        mine = slice(owner * seqs, (owner + 1) * seqs)
        high = wide[mine].astype(bf16).astype(f32)
        sums = jnp.where(lane < 64, high, wide[mine] - high)
        send_a[owner, :, 3 * key_width :] = sums.astype(bf16)
    project("q", wq_ref, send_a, 0)
    project("k", wk_ref, send_a, key_width)
    project("d", wd_ref, send_a, 2 * key_width)

    @pl.when(tp == 0)
    def _():
        pl.semaphore_wait(go_sem, 1)

    send_group(0)
    project("v", wv_ref, send_b, 0)
    send_group(1)
    project("g", wg_ref, send_c, 0)
    send_group(2)

    w_out_copy = remote(w_out_hbm, w_out_other, w_out_sem.at[0], w_out_sem.at[1], kv, 1)

    @pl.when(tp == 0)
    def _():
        w_out_copy.start()

    def gathered(group):
        send, recv = groups[group]
        total = send[kv].astype(f32)
        for j in near:
            proj_copy(group, j, j).wait_recv()
        for j in near:
            total = total + recv[j].astype(f32)
        return total

    group_a = gathered(0)
    row_sums = group_a[:, 3 * key_width : 3 * key_width + 1] + group_a[:, 3 * key_width + 64 : 3 * key_width + 65]
    row_scale = lax.rsqrt(row_sums * (1.0 / width) + epsilon)
    queries = group_a[:, :key_width] * (row_scale * key_dim**-0.5)
    new_keys = group_a[:, key_width : 2 * key_width] * row_scale
    retain = jax.nn.sigmoid(
        group_a[:, 2 * key_width : 3 * key_width] * row_scale + decay_offset_ref[...]
    )
    query_retain = queries * retain
    overlap = queries * new_keys
    for h in range(heads):
        cols = slice(h * key_dim, (h + 1) * key_dim)
        coef[(3 * h) * seqs : (3 * h + 1) * seqs, :] = query_retain[:, cols]
        coef[(3 * h + 1) * seqs : (3 * h + 2) * seqs, :] = new_keys[:, cols]
        coef[(3 * h + 2) * seqs : (3 * h + 3) * seqs, :] = retain[:, cols]
    coef_t[...] = coef[...].T
    loads["state"].wait()
    for h in range(heads):
        for b in range(seqs):
            at = 3 * h * seqs + b
            total = jnp.zeros((8, val_dim), f32)
            for start in range(0, key_dim, ROW_CHUNK):
                piece = slice(start, start + ROW_CHUNK)
                product = coef_t[piece, at : at + 1] * state_ref[b, h, piece, :]
                total = total + jnp.sum(product.reshape(ROW_CHUNK // 8, 8, val_dim), axis=0)
            read[h, b : b + 1, :] = jnp.sum(total, axis=0, keepdims=True)

    values = gathered(1) * row_scale
    vals[...] = values
    gates = gathered(2) * row_scale
    for h in range(heads):
        cols = slice(h * val_dim, (h + 1) * val_dim)
        dots = jnp.sum(overlap[:, h * key_dim : (h + 1) * key_dim], axis=1, keepdims=True)
        readout = read[h] + dots * values[:, cols]
        mean = jnp.mean(readout * readout, axis=1, keepdims=True)
        gate = gates[:, cols]
        gated_all[tp, kv, :, cols] = (
            readout * lax.rsqrt(mean + epsilon) * head_gain_ref[...] * (gate * jax.nn.sigmoid(gate))
        ).astype(bf16)

    def gated_copy(j, from_tp, from_kv):
        block = gated_all.at[from_tp, from_kv]
        return remote(
            block, block, gated_send_sem.at[j], gated_recv_sem.at[from_tp, from_kv], j, 1
        )

    for j in far:
        gated_copy(j, tp, kv).start()

    @pl.when(tp == 0)
    def _():
        gated_copy(kv, 0, kv).start()

    for h in range(heads):
        for b in range(seqs):
            at = 3 * h * seqs + b
            value_row = vals[b : b + 1, h * val_dim : (h + 1) * val_dim]
            for start in range(0, key_dim, ROW_CHUNK):
                piece = slice(start, start + ROW_CHUNK)
                state_ref[b, h, piece, :] = (
                    coef_t[piece, at + 2 * seqs : at + 2 * seqs + 1] * state_ref[b, h, piece, :]
                    + coef_t[piece, at + seqs : at + seqs + 1] * value_row
                )

    tok_copy.wait_send()
    for group in range(3):
        for j in far:
            proj_copy(group, j, kv).wait_send()

    def stream_copy(j, to_tp, owner):
        block = stream_all.at[owner]
        return remote(block, block, stream_send_sem.at[j, to_tp], stream_recv_sem.at[owner], j, to_tp)

    def out_rows(from_tp):
        for owner in range(n_kv):
            gated_rows[owner * seqs : (owner + 1) * seqs, :] = gated_all[from_tp, owner].astype(f32)
        return gated_rows[...].astype(bf16)

    @pl.when(tp == 1)
    def _():
        for j in near:
            gated_copy(kv, 1, j).wait_recv()
        loads["out"].wait()
        branch = jnp.dot(out_rows(1), w_out_ref[...], preferred_element_type=f32)
        w_out_copy.wait_recv()
        for j in [kv] + near:
            gated_copy(kv, 0, j).wait_recv()
        branch = branch + jnp.dot(out_rows(0), w_out_other[...], preferred_element_type=f32)
        for i in range(2):
            stream_all[kv, i] = (tok_all[i].astype(f32) + branch[:, i * half : (i + 1) * half]).astype(bf16)
        for j in far:
            for to_tp in range(2):
                stream_copy(j, to_tp, kv).start()
        stream_copy(kv, 0, kv).start()

    for j in far:
        gated_copy(j, tp, kv).wait_send()

    loads["up"].wait()

    @pl.when(tp == 0)
    def _():
        gated_copy(kv, 0, kv).wait_send()
        w_out_copy.wait_send()
        stream_copy(kv, 0, kv).wait_recv()

    hidden = None
    sums = None
    for step, owner in enumerate([kv] + near):
        if step > 0:
            stream_copy(kv, tp, owner).wait_recv()
        pieces = [stream_all[owner, i].astype(f32) for i in range(2)]
        normed = jnp.concatenate(
            [(piece * mlp_gain_ref[owner, i]).astype(bf16) for i, piece in enumerate(pieces)], axis=1
        )
        first = pl.multiple_of(owner * (2 * half), 2 * half)
        term = jnp.dot(normed, w_up_ref[pl.ds(first, 2 * half), :], preferred_element_type=f32)
        part = sum(jnp.sum(piece * piece, axis=1, keepdims=True) for piece in pieces)
        hidden = term if hidden is None else hidden + term
        sums = part if sums is None else sums + part
        if step == 0:
            loads["down"].wait()
    mlp_scale = lax.rsqrt(sums * (1.0 / width) + epsilon)
    active = jnp.maximum(hidden * mlp_scale, 0.0)
    squared = (active * active).astype(bf16)

    def down_copy(at, j, to_tp, slot):
        return remote(
            down_send.at[at, to_tp], down_recv.at[slot], down_send_sem.at[at, to_tp], down_recv_sem.at[slot], j, to_tp
        )

    me = 2 * kv + tp
    for at, j in enumerate(far + [kv]):
        first = pl.multiple_of(j * (2 * half), 2 * half)
        term = jnp.dot(squared, w_down_ref[:, pl.ds(first, 2 * half)], preferred_element_type=f32)
        for i in range(2):
            down_send[at, i] = term[:, i * half : (i + 1) * half].astype(bf16)
            if at == n_kv - 1:
                down_own[i] = term[:, i * half : (i + 1) * half]
        if at < n_kv - 1:
            for i in range(2):
                down_copy(at, j, i, me).start()
        else:
            down_copy(at, kv, other, me).start()
    total = stream_all[kv, tp].astype(f32) + down_own[tp]

    @pl.when(tp == 1)
    def _():
        for j in far:
            for to_tp in range(2):
                stream_copy(j, to_tp, kv).wait_send()
        stream_copy(kv, 0, kv).wait_send()

    slots = [2 * kv + other] + [2 * j + i for j in near for i in range(2)]
    for slot in slots:
        down_copy(0, kv, tp, slot).wait_recv()
        total = total + down_recv[slot].astype(f32)
    mixed_ref[...] = total.astype(bf16)
    for at, j in enumerate(far):
        for i in range(2):
            down_copy(at, j, i, me).wait_send()
    down_copy(n_kv - 1, kv, other, me).wait_send()


def write_kernel(mixed_ref, state_ref, mixed_hbm, state_hbm, state_sem, mixed_sem):
    seqs, heads = state_ref.shape[:2]
    copies = [pltpu.make_async_copy(mixed_ref, mixed_hbm, mixed_sem.at[0])]
    for b in range(seqs):
        for h in range(heads):
            copies.append(
                pltpu.make_async_copy(state_ref.at[b, h], state_hbm.at[b, h], state_sem.at[b, h])
            )
    for copy in copies:
        copy.start()
    for copy in copies:
        copy.wait()


def kernel_shards(
    n_kv,
    tokens,
    state,
    mix_gain,
    w_query,
    w_key,
    w_decay,
    w_value,
    w_gate,
    decay_offset,
    head_gain,
    w_out,
    mlp_gain,
    w_up,
    w_down,
):
    f32, bf16 = jnp.float32, jnp.bfloat16
    rows, half = tokens.shape
    seqs, heads, key_dim, val_dim = state.shape
    key_width, val_width = heads * key_dim, heads * val_dim
    vmem = pl.BlockSpec(memory_space=pltpu.VMEM)
    hbm = pl.BlockSpec(memory_space=pltpu.HBM)
    weights = (w_query, w_key, w_decay, w_value, w_gate, w_out, w_up, w_down)
    a_width = 3 * key_width + 128
    coef_rows = 3 * heads * seqs
    coef_rows += -coef_rows % 8
    dma = pltpu.SemaphoreType.DMA
    regular = pltpu.SemaphoreType.REGULAR
    scratch = (
        [
            pltpu.VMEM(tokens.shape, bf16),
            pltpu.VMEM((2, 1, half), f32),
            pltpu.VMEM((1, key_width), f32),
            pltpu.VMEM((1, val_dim), f32),
            pltpu.VMEM((n_kv, 2, 1, half), f32),
        ]
        + [pltpu.VMEM(weight.shape, bf16) for weight in weights]
        + [
            pltpu.VMEM(w_out.shape, bf16),
            pltpu.VMEM((2, rows, half), bf16),
            pltpu.VMEM((n_kv, seqs, a_width), bf16),
            pltpu.VMEM((n_kv, seqs, val_width), bf16),
            pltpu.VMEM((n_kv, seqs, val_width), bf16),
            pltpu.VMEM((n_kv, seqs, a_width), bf16),
            pltpu.VMEM((n_kv, seqs, val_width), bf16),
            pltpu.VMEM((n_kv, seqs, val_width), bf16),
            pltpu.VMEM((coef_rows, key_dim), f32),
            pltpu.VMEM((key_dim, coef_rows), f32),
            pltpu.VMEM((seqs, val_width), f32),
            pltpu.VMEM((heads, seqs, val_dim), f32),
            pltpu.VMEM((2, n_kv, seqs, val_width), bf16),
            pltpu.VMEM((rows, val_width), f32),
            pltpu.VMEM((n_kv, 2, rows, half), bf16),
            pltpu.VMEM((n_kv, 2, rows, half), bf16),
            pltpu.VMEM((2, rows, half), f32),
            pltpu.VMEM((2 * n_kv, rows, half), bf16),
            dma((14,)),
            regular,
            regular,
            dma((2,)),
            dma((2,)),
            dma((3, n_kv)),
            dma((3, n_kv)),
            dma((n_kv,)),
            dma((2, n_kv)),
            dma((n_kv, 2)),
            dma((n_kv,)),
            dma((n_kv, 2)),
            dma((2 * n_kv,)),
        ]
    )
    mixed, new_state = pl.pallas_call(
        functools.partial(layer_kernel, n_kv),
        out_shape=(
            pltpu.VMEM(tokens.shape, bf16),
            pltpu.VMEM(state.shape, f32),
        ),
        in_specs=[hbm] * 14,
        out_specs=(vmem, vmem),
        scratch_shapes=scratch,
        compiler_params=pltpu.CompilerParams(
            collective_id=0, has_side_effects=True, vmem_limit_bytes=VMEM_BYTES - 4 * state.size - 2**19
        ),
    )(
        tokens,
        mix_gain.reshape(2, 1, half),
        decay_offset.reshape(1, key_width),
        head_gain.reshape(1, val_dim),
        mlp_gain.reshape(n_kv, 2, 1, half),
        state,
        *weights,
    )
    return pl.pallas_call(
        write_kernel,
        out_shape=(
            jax.ShapeDtypeStruct(tokens.shape, bf16),
            jax.ShapeDtypeStruct(state.shape, f32),
        ),
        in_specs=[vmem] * 2,
        out_specs=(hbm, hbm),
        scratch_shapes=[dma((seqs, heads)), dma((1,))],
        compiler_params=pltpu.CompilerParams(vmem_limit_bytes=2**20),
    )(
        pltpu.with_memory_space_constraint(mixed, pltpu.VMEM),
        pltpu.with_memory_space_constraint(new_state, pltpu.VMEM),
    )


def fits_kernel(mesh):
    n_kv, n_tp = mesh.shape["kv"], mesh.shape["tp"]
    return n_tp == 2 and n_kv > 1 and D % (128 * n_kv * n_tp) == 0


def solution(mesh):
    in_specs = (
        P("dp", ("kv", "tp")),
        P(("dp", "kv"), "tp", None, None),
        P("kv"),
        P("kv", "tp"),
        P("kv", "tp"),
        P("kv", "tp"),
        P("kv", "tp"),
        P("kv", "tp"),
        P("tp"),
        P(),
        P("tp", "kv"),
        P(),
        P(None, ("kv", "tp")),
        P(("kv", "tp"), None),
    )
    out_specs = (P("dp", ("kv", "tp")), P(("dp", "kv"), "tp", None, None))
    shards = plain_shards
    if fits_kernel(mesh):
        shards = functools.partial(kernel_shards, mesh.shape["kv"])
    return jax.shard_map(shards, mesh=mesh, in_specs=in_specs, out_specs=out_specs, check_vma=False)
```

```python
import functools

import jax
import jax.numpy as jnp
from jax import lax
from jax.experimental import pallas as pl
from jax.experimental.pallas import tpu as pltpu
from jax.sharding import PartitionSpec as P

D = 2048


epsilon = 1e-06


def plain_shards(
    tokens,
    state,
    mix_gain,
    w_query,
    w_key,
    w_decay,
    w_value,
    w_gate,
    decay_offset,
    head_gain,
    w_out,
    mlp_gain,
    w_up,
    w_down,
):
    seq_dev = state.shape[0]
    heads_here = state.shape[1]
    key_dim = state.shape[2]
    val_dim = state.shape[3]
    weights = (w_query, w_key, w_decay, w_value, w_gate)
    tok_cols = lax.all_gather(tokens, "tp", axis=1, tiled=True)
    tok_float = tok_cols.astype(jnp.float32)
    squares = jnp.sum(tok_float * tok_float, axis=1)
    scaled = (tok_float * mix_gain).astype(jnp.bfloat16)
    kv_index = lax.axis_index("kv")
    projected = lax.psum_scatter(
        jnp.concatenate(
            [jnp.dot(scaled, weight, preferred_element_type=jnp.float32) for weight in weights],
            axis=1,
        ),
        "kv",
        scatter_dimension=0,
        tiled=True,
    )
    all_sums = lax.psum(squares, "kv")
    row_sums = lax.dynamic_slice_in_dim(all_sums, kv_index * seq_dev, seq_dev, 0)
    row_scale = lax.rsqrt(row_sums / D + epsilon)[:, None]
    projected = projected * row_scale
    key_width = heads_here * key_dim
    val_width = heads_here * val_dim
    queries = (projected[:, :key_width] * key_dim ** (-0.5)).reshape(seq_dev, heads_here, key_dim)
    new_keys = projected[:, key_width : 2 * key_width].reshape(seq_dev, heads_here, key_dim)
    retain = jax.nn.sigmoid(projected[:, 2 * key_width : 3 * key_width] + decay_offset).reshape(
        seq_dev, heads_here, key_dim
    )
    values = projected[:, 3 * key_width : 3 * key_width + val_width].reshape(
        seq_dev, heads_here, val_dim
    )
    gates = projected[:, 3 * key_width + val_width :]
    new_state = retain[..., None] * state + new_keys[..., None] * values[:, :, None, :]
    readout = jnp.einsum("bhk,bhkv->bhv", queries, new_state, precision=lax.Precision.HIGHEST)
    readout = (
        readout
        * lax.rsqrt(jnp.mean(readout * readout, axis=2, keepdims=True) + epsilon)
        * head_gain
    )
    gated = (readout.reshape(seq_dev, val_width) * jax.nn.silu(gates)).astype(jnp.bfloat16)
    branch = jnp.dot(
        lax.all_gather(gated, "kv", axis=0, tiled=True), w_out, preferred_element_type=jnp.float32
    )
    own_width = tokens.shape[1]
    branch_total = lax.psum(branch.astype(jnp.bfloat16), "tp").astype(jnp.float32)
    stream_cols = (tok_float + branch_total).astype(jnp.bfloat16)
    stream = lax.all_gather(stream_cols, "kv", axis=1, tiled=True)
    stream_own = lax.dynamic_slice_in_dim(
        stream_cols, lax.axis_index("tp") * own_width, own_width, 1
    )
    stream_float = stream.astype(jnp.float32)
    mlp_scale = lax.rsqrt(jnp.mean(stream_float * stream_float, axis=1, keepdims=True) + epsilon)
    normed = (stream_float * mlp_gain).astype(jnp.bfloat16)
    hidden = jnp.dot(normed, w_up, preferred_element_type=jnp.float32) * mlp_scale
    squared = jnp.square(jax.nn.relu(hidden)).astype(jnp.bfloat16)
    down_own = lax.psum_scatter(
        lax.dot_general(
            w_down, squared, (((0,), (1,)), ((), ())), preferred_element_type=jnp.float32
        ),
        ("kv", "tp"),
        scatter_dimension=0,
        tiled=True,
    )
    mixed = (stream_own.astype(jnp.float32) + down_own.T).astype(jnp.bfloat16)
    return (mixed, new_state)


MESH = pl.DeviceIdType.MESH
ROW_CHUNK = 64
VMEM_BYTES = 67_043_328


def pick(index, values):
    chosen = values[0]
    for at in range(1, len(values)):
        chosen = jnp.where(index == at, values[at], chosen)
    return chosen


def far_first(n_kv, kv):
    orders = [
        sorted((j for j in range(n_kv) if j != me), key=lambda j: (-abs(j - me), j)) for me in range(n_kv)
    ]
    return [pick(kv, [order[at] for order in orders]) for at in range(n_kv - 1)]


def layer_kernel(
    n_kv,
    tok_hbm,
    mix_gain_hbm,
    decay_offset_hbm,
    head_gain_hbm,
    mlp_gain_hbm,
    state_hbm,
    wq_hbm,
    wk_hbm,
    wd_hbm,
    wv_hbm,
    wg_hbm,
    w_out_hbm,
    w_up_hbm,
    w_down_hbm,
    mixed_ref,
    state_ref,
    tok_ref,
    mix_gain_ref,
    decay_offset_ref,
    head_gain_ref,
    mlp_gain_ref,
    w_qkd_ref,
    wv_ref,
    wg_ref,
    w_out_ref,
    w_up_ref,
    w_down_ref,
    w_out_other,
    tok_all,
    send_a,
    send_b,
    send_c,
    recv_a,
    recv_b,
    recv_c,
    coef,
    coef_t,
    vals,
    read,
    gated_all,
    gated_rows,
    stream_all,
    down_send,
    down_own,
    down_recv,
    load_sem,
    ready_sem,
    tok_sem,
    w_out_sem,
    proj_sem,
    gated_sem,
    stream_send_sem,
    stream_recv_sem,
    down_sem,
):
    f32, bf16 = jnp.float32, jnp.bfloat16
    kv, tp = lax.axis_index("kv"), lax.axis_index("tp")
    other = 1 - tp
    rows, half = tok_ref.shape
    seqs, heads, key_dim, val_dim = state_ref.shape
    key_width, val_width = heads * key_dim, heads * val_dim
    width = 2 * n_kv * half
    far = far_first(n_kv, kv)
    near = far[::-1]

    def remote(src, dst, send_sem, recv_sem, to_kv, to_tp):
        return pltpu.make_async_remote_copy(
            src_ref=src,
            dst_ref=dst,
            send_sem=send_sem,
            recv_sem=recv_sem,
            device_id={"kv": to_kv, "tp": to_tp},
            device_id_type=MESH,
        )

    def signal(sem, to_kv, to_tp):
        pl.semaphore_signal(sem, inc=1, device_id={"kv": to_kv, "tp": to_tp}, device_id_type=MESH)

    barrier = pltpu.get_barrier_semaphore()

    @pl.when(tp == 1)
    def _():
        signal(barrier, kv, 0)

    for j in far:
        signal(barrier, j, 1)

        @pl.when(j > kv)
        def _():
            signal(barrier, j, 0)

    loads = {}
    at_sem = {}
    for name, source, target in (
        ("tokens", tok_hbm, tok_ref),
        ("mix_gain", mix_gain_hbm, mix_gain_ref),
        ("q", wq_hbm, w_qkd_ref.at[0]),
        ("k", wk_hbm, w_qkd_ref.at[1]),
        ("d", wd_hbm, w_qkd_ref.at[2]),
        ("offset", decay_offset_hbm, decay_offset_ref),
        ("head_gain", head_gain_hbm, head_gain_ref),
        ("mlp_gain", mlp_gain_hbm, mlp_gain_ref),
        ("v", wv_hbm, wv_ref),
        ("g", wg_hbm, wg_ref),
        ("state", state_hbm, state_ref),
        ("up", w_up_hbm, w_up_ref),
        ("down", w_down_hbm, w_down_ref),
        ("out", w_out_hbm, w_out_ref),
    ):
        group = "q" if name in ("k", "d") else name
        sem = load_sem.at[at_sem.setdefault(group, len(at_sem))]
        loads[name] = pltpu.make_async_copy(source, target, sem)
        if name != "out":
            loads[name].start()
    loads["q"] = pltpu.make_async_copy(w_qkd_ref, w_qkd_ref, load_sem.at[at_sem["q"]])

    @pl.when(tp == 0)
    def _():
        pl.semaphore_wait(barrier, 1 + 2 * kv)
        signal(ready_sem, kv, 1)

    @pl.when(tp == 1)
    def _():
        loads["out"].start()
        pl.semaphore_wait(ready_sem, 1)

    loads["tokens"].wait()
    tok_copy = remote(tok_ref, tok_all.at[tp], tok_sem.at[0], tok_sem.at[1], kv, other)
    tok_copy.start()
    tok_all[tp] = tok_ref[...]
    tok_own = tok_ref[...].astype(f32)
    squares = jnp.sum(tok_own * tok_own, axis=1, keepdims=True)
    loads["mix_gain"].wait()

    def half_rows(which):
        return pl.ds(pl.multiple_of(which * half, half), half)

    scaled_own = (tok_own * mix_gain_ref[tp]).astype(bf16)
    loads["q"].wait()
    early = [
        jnp.dot(scaled_own, w_qkd_ref[i, half_rows(tp), :], preferred_element_type=f32) for i in range(3)
    ]
    tok_copy.wait_recv()
    tok_other = tok_all[other].astype(f32)
    squares = squares + jnp.sum(tok_other * tok_other, axis=1, keepdims=True)
    scaled_other = (tok_other * mix_gain_ref[other]).astype(bf16)

    groups = ((send_a, recv_a), (send_b, recv_b), (send_c, recv_c))

    def fill(send, total, at):
        columns = total.shape[1]
        for owner in range(n_kv):
            send[owner, :, at : at + columns] = total[owner * seqs : (owner + 1) * seqs].astype(bf16)

    def project(name, weight_ref, send):
        loads[name].wait()
        total = jnp.dot(scaled_own, weight_ref[half_rows(tp), :], preferred_element_type=f32)
        fill(send, total + jnp.dot(scaled_other, weight_ref[half_rows(other), :], preferred_element_type=f32), 0)

    def proj_copy(group, j):
        send, recv = groups[group]
        return remote(send.at[j], recv.at[kv], proj_sem.at[group, 0], proj_sem.at[group, 1], j, tp)

    def proj_all(group):
        send, recv = groups[group]
        some = pl.ds(0, n_kv - 1)
        return remote(send.at[some], recv.at[some], proj_sem.at[group, 0], proj_sem.at[group, 1], kv, other)

    def send_lower(group):
        for j in far:

            @pl.when(j < kv)
            def _():
                proj_copy(group, j).start()

    def send_higher():
        order = sorted(
            ((group, at) for group in range(3) for at in range(n_kv - 1)),
            key=lambda item: item[1] * 2 + (0 if item[0] == 0 else 3),
        )
        for group, at in order:

            @pl.when(far[at] > kv)
            def _():
                proj_copy(group, far[at]).start()

    wide = jnp.broadcast_to(squares, (rows, 128))
    lane = lax.broadcasted_iota(jnp.int32, (seqs, 128), 1)
    for owner in range(n_kv):
        mine = slice(owner * seqs, (owner + 1) * seqs)
        high = wide[mine].astype(bf16).astype(f32)
        sums = jnp.where(lane < 64, high, wide[mine] - high)
        send_a[owner, :, 3 * key_width :] = sums.astype(bf16)
    late = [
        jnp.dot(scaled_other, w_qkd_ref[i, half_rows(other), :], preferred_element_type=f32) for i in range(3)
    ]
    for i in range(3):
        fill(send_a, early[i] + late[i], i * key_width)
    send_lower(0)
    project("v", wv_ref, send_b)
    send_lower(1)

    @pl.when(tp == 1)
    def _():
        pl.semaphore_wait(barrier, 2 * (n_kv - 1))
        signal(ready_sem, kv, 0)

    project("g", wg_ref, send_c)
    send_lower(2)

    @pl.when(tp == 0)
    def _():
        pl.semaphore_wait(ready_sem, 1)

    send_higher()

    w_out_copy = remote(w_out_hbm, w_out_other, w_out_sem, w_out_sem, kv, 1)

    @pl.when(tp == 0)
    def _():
        w_out_copy.start()

    def gathered(group):
        send, recv = groups[group]
        total = send[kv].astype(f32)
        proj_all(group).wait_recv()
        for j in near:
            total = total + recv[j].astype(f32)
        return total

    group_a = gathered(0)
    row_sums = group_a[:, 3 * key_width : 3 * key_width + 1] + group_a[:, 3 * key_width + 64 : 3 * key_width + 65]
    row_scale = lax.rsqrt(row_sums * (1.0 / width) + epsilon)
    queries = group_a[:, :key_width] * (row_scale * key_dim**-0.5)
    new_keys = group_a[:, key_width : 2 * key_width] * row_scale
    loads["offset"].wait()
    retain = jax.nn.sigmoid(
        group_a[:, 2 * key_width : 3 * key_width] * row_scale + decay_offset_ref[...]
    )
    query_retain = queries * retain
    overlap = queries * new_keys
    for h in range(heads):
        cols = slice(h * key_dim, (h + 1) * key_dim)
        coef[(3 * h) * seqs : (3 * h + 1) * seqs, :] = query_retain[:, cols]
        coef[(3 * h + 1) * seqs : (3 * h + 2) * seqs, :] = new_keys[:, cols]
        coef[(3 * h + 2) * seqs : (3 * h + 3) * seqs, :] = retain[:, cols]
    coef_t[...] = coef[...].T
    loads["state"].wait()
    for h in range(heads):
        for b in range(seqs):
            at = 3 * h * seqs + b
            total = jnp.zeros((8, val_dim), f32)
            for start in range(0, key_dim, ROW_CHUNK):
                piece = slice(start, start + ROW_CHUNK)
                product = coef_t[piece, at : at + 1] * state_ref[b, h, piece, :]
                total = total + jnp.sum(product.reshape(ROW_CHUNK // 8, 8, val_dim), axis=0)
            read[h, b : b + 1, :] = jnp.sum(total, axis=0, keepdims=True)

    values = gathered(1) * row_scale
    vals[...] = values
    gates = gathered(2) * row_scale
    loads["head_gain"].wait()
    for h in range(heads):
        cols = slice(h * val_dim, (h + 1) * val_dim)
        dots = jnp.sum(overlap[:, h * key_dim : (h + 1) * key_dim], axis=1, keepdims=True)
        readout = read[h] + dots * values[:, cols]
        mean = jnp.mean(readout * readout, axis=1, keepdims=True)
        gate = gates[:, cols]
        gated_all[tp, kv, :, cols] = (
            readout * lax.rsqrt(mean + epsilon) * head_gain_ref[...] * (gate * jax.nn.sigmoid(gate))
        ).astype(bf16)

    def gated_copy(j):
        block = gated_all.at[tp, kv]
        return remote(block, block, gated_sem.at[0], gated_sem.at[1 + tp], j, 1)

    def gated_some(from_tp, count):
        blocks = gated_all.at[from_tp, pl.ds(0, count)]
        return remote(blocks, blocks, gated_sem.at[0], gated_sem.at[1 + from_tp], kv, other)

    for j in far:
        gated_copy(j).start()

    @pl.when(tp == 0)
    def _():
        gated_copy(kv).start()

    for h in range(heads):
        for b in range(seqs):
            at = 3 * h * seqs + b
            value_row = vals[b : b + 1, h * val_dim : (h + 1) * val_dim]
            for start in range(0, key_dim, ROW_CHUNK):
                piece = slice(start, start + ROW_CHUNK)
                state_ref[b, h, piece, :] = (
                    coef_t[piece, at + 2 * seqs : at + 2 * seqs + 1] * state_ref[b, h, piece, :]
                    + coef_t[piece, at + seqs : at + seqs + 1] * value_row
                )

    tok_copy.wait_send()
    for group in range(3):
        proj_all(group).wait_send()

    def stream_copy(j, to_tp, owner):
        block = stream_all.at[owner]
        return remote(block, block, stream_send_sem.at[to_tp], stream_recv_sem.at[owner], j, to_tp)

    def out_rows(from_tp):
        for owner in range(n_kv):
            gated_rows[owner * seqs : (owner + 1) * seqs, :] = gated_all[from_tp, owner].astype(f32)
        return gated_rows[...].astype(bf16)

    @pl.when(tp == 1)
    def _():
        gated_some(1, n_kv - 1).wait_recv()
        loads["out"].wait()
        branch = jnp.dot(out_rows(1), w_out_ref[...], preferred_element_type=f32)
        w_out_copy.wait_recv()
        gated_some(0, n_kv).wait_recv()
        branch = branch + jnp.dot(out_rows(0), w_out_other[...], preferred_element_type=f32)
        for i in range(2):
            stream_all[kv, i] = (tok_all[i].astype(f32) + branch[:, i * half : (i + 1) * half]).astype(bf16)
        for j in far:
            for to_tp in range(2):
                stream_copy(j, to_tp, kv).start()
        stream_copy(kv, 0, kv).start()

        gated_some(1, n_kv - 1).wait_send()

    loads["mlp_gain"].wait()
    loads["up"].wait()

    @pl.when(tp == 0)
    def _():
        gated_some(0, n_kv).wait_send()
        w_out_copy.wait_send()
        stream_copy(kv, 0, kv).wait_recv()

    hidden = None
    sums = None
    for step, owner in enumerate([kv] + near):
        if step > 0:
            stream_copy(kv, tp, owner).wait_recv()
        pieces = [stream_all[owner, i].astype(f32) for i in range(2)]
        normed = jnp.concatenate(
            [(piece * mlp_gain_ref[owner, i]).astype(bf16) for i, piece in enumerate(pieces)], axis=1
        )
        first = pl.multiple_of(owner * (2 * half), 2 * half)
        term = jnp.dot(normed, w_up_ref[pl.ds(first, 2 * half), :], preferred_element_type=f32)
        part = sum(jnp.sum(piece * piece, axis=1, keepdims=True) for piece in pieces)
        hidden = term if hidden is None else hidden + term
        sums = part if sums is None else sums + part
        if step == 0:
            loads["down"].wait()
    mlp_scale = lax.rsqrt(sums * (1.0 / width) + epsilon)
    active = jnp.maximum(hidden * mlp_scale, 0.0)
    squared = (active * active).astype(bf16)

    def down_copy(at, j, to_tp):
        return remote(down_send.at[at, to_tp], down_recv.at[2 * kv + tp], down_sem.at[0], down_sem.at[1], j, to_tp)

    def down_columns(first, columns):
        return jnp.dot(
            squared, w_down_ref[:, pl.ds(pl.multiple_of(first, half), columns)], preferred_element_type=f32
        )

    for at, j in enumerate(far):
        if at == 0:
            for i in range(2):
                down_send[at, i] = down_columns((2 * j + i) * half, half).astype(bf16)
                down_copy(at, j, i).start()
        else:
            term = down_columns(2 * j * half, 2 * half)
            for i in range(2):
                down_send[at, i] = term[:, i * half : (i + 1) * half].astype(bf16)
                down_copy(at, j, i).start()
    term = down_columns(2 * kv * half, 2 * half)
    for i in range(2):
        down_own[i] = term[:, i * half : (i + 1) * half]
        down_send[n_kv - 1, i] = term[:, i * half : (i + 1) * half].astype(bf16)
    down_copy(n_kv - 1, kv, other).start()
    total = stream_all[kv, tp].astype(f32) + down_own[tp]

    @pl.when(tp == 1)
    def _():
        remote(stream_all, stream_all, stream_send_sem.at[0], stream_recv_sem.at[0], kv, 0).wait_send()
        some = stream_all.at[pl.ds(0, n_kv - 1)]
        remote(some, some, stream_send_sem.at[1], stream_recv_sem.at[0], kv, 0).wait_send()

    some = down_recv.at[pl.ds(0, 2 * n_kv - 1)]
    down_all = remote(some, some, down_sem.at[0], down_sem.at[1], kv, other)
    down_all.wait_recv()
    for slot in [2 * kv + other] + [2 * j + i for j in near for i in range(2)]:
        total = total + down_recv[slot].astype(f32)
    mixed_ref[...] = total.astype(bf16)
    down_all.wait_send()


def write_kernel(mixed_ref, state_ref, mixed_hbm, state_hbm, state_sem, mixed_sem):
    seqs, heads = state_ref.shape[:2]
    copies = [pltpu.make_async_copy(mixed_ref, mixed_hbm, mixed_sem.at[0])]
    for b in range(seqs):
        for h in range(heads):
            copies.append(
                pltpu.make_async_copy(state_ref.at[b, h], state_hbm.at[b, h], state_sem.at[b, h])
            )
    for copy in copies:
        copy.start()
    for copy in copies:
        copy.wait()


def kernel_shards(
    n_kv,
    tokens,
    state,
    mix_gain,
    w_query,
    w_key,
    w_decay,
    w_value,
    w_gate,
    decay_offset,
    head_gain,
    w_out,
    mlp_gain,
    w_up,
    w_down,
):
    f32, bf16 = jnp.float32, jnp.bfloat16
    rows, half = tokens.shape
    seqs, heads, key_dim, val_dim = state.shape
    key_width, val_width = heads * key_dim, heads * val_dim
    vmem = pl.BlockSpec(memory_space=pltpu.VMEM)
    hbm = pl.BlockSpec(memory_space=pltpu.HBM)
    weights = (w_query, w_key, w_decay, w_value, w_gate, w_out, w_up, w_down)
    a_width = 3 * key_width + 128
    coef_rows = 3 * heads * seqs
    coef_rows += -coef_rows % 8
    dma = pltpu.SemaphoreType.DMA
    scratch = (
        [
            pltpu.VMEM(tokens.shape, bf16),
            pltpu.VMEM((2, 1, half), f32),
            pltpu.VMEM((1, key_width), f32),
            pltpu.VMEM((1, val_dim), f32),
            pltpu.VMEM((n_kv, 2, 1, half), f32),
        ]
        + [pltpu.VMEM((3,) + w_query.shape, bf16)]
        + [pltpu.VMEM(weight.shape, bf16) for weight in weights[3:]]
        + [
            pltpu.VMEM(w_out.shape, bf16),
            pltpu.VMEM((2, rows, half), bf16),
            pltpu.VMEM((n_kv, seqs, a_width), bf16),
            pltpu.VMEM((n_kv, seqs, val_width), bf16),
            pltpu.VMEM((n_kv, seqs, val_width), bf16),
            pltpu.VMEM((n_kv, seqs, a_width), bf16),
            pltpu.VMEM((n_kv, seqs, val_width), bf16),
            pltpu.VMEM((n_kv, seqs, val_width), bf16),
            pltpu.VMEM((coef_rows, key_dim), f32),
            pltpu.VMEM((key_dim, coef_rows), f32),
            pltpu.VMEM((seqs, val_width), f32),
            pltpu.VMEM((heads, seqs, val_dim), f32),
            pltpu.VMEM((2, n_kv, seqs, val_width), bf16),
            pltpu.VMEM((rows, val_width), f32),
            pltpu.VMEM((n_kv, 2, rows, half), bf16),
            pltpu.VMEM((n_kv, 2, rows, half), bf16),
            pltpu.VMEM((2, rows, half), f32),
            pltpu.VMEM((2 * n_kv, rows, half), bf16),
            dma((12,)),
            pltpu.SemaphoreType.REGULAR,
            dma((2,)),
            dma,
            dma((3, 2)),
            dma((3,)),
            dma((2,)),
            dma((n_kv,)),
            dma((2,)),
        ]
    )
    mixed, new_state = pl.pallas_call(
        functools.partial(layer_kernel, n_kv),
        out_shape=(
            pltpu.VMEM(tokens.shape, bf16),
            pltpu.VMEM(state.shape, f32),
        ),
        in_specs=[hbm] * 14,
        out_specs=(vmem, vmem),
        scratch_shapes=scratch,
        compiler_params=pltpu.CompilerParams(
            collective_id=0, has_side_effects=True, vmem_limit_bytes=VMEM_BYTES - 4 * state.size - 2**19
        ),
    )(
        tokens,
        mix_gain.reshape(2, 1, half),
        decay_offset.reshape(1, key_width),
        head_gain.reshape(1, val_dim),
        mlp_gain.reshape(n_kv, 2, 1, half),
        state,
        *weights,
    )
    return pl.pallas_call(
        write_kernel,
        out_shape=(
            jax.ShapeDtypeStruct(tokens.shape, bf16),
            jax.ShapeDtypeStruct(state.shape, f32),
        ),
        in_specs=[vmem] * 2,
        out_specs=(hbm, hbm),
        scratch_shapes=[dma((seqs, heads)), dma((1,))],
        compiler_params=pltpu.CompilerParams(vmem_limit_bytes=2**20),
    )(
        pltpu.with_memory_space_constraint(mixed, pltpu.VMEM),
        pltpu.with_memory_space_constraint(new_state, pltpu.VMEM),
    )


def fits_kernel(mesh):
    n_kv, n_tp = mesh.shape["kv"], mesh.shape["tp"]
    return n_tp == 2 and n_kv > 1 and D % (128 * n_kv * n_tp) == 0


def solution(mesh):
    in_specs = (
        P("dp", ("kv", "tp")),
        P(("dp", "kv"), "tp", None, None),
        P("kv"),
        P("kv", "tp"),
        P("kv", "tp"),
        P("kv", "tp"),
        P("kv", "tp"),
        P("kv", "tp"),
        P("tp"),
        P(),
        P("tp", "kv"),
        P(),
        P(None, ("kv", "tp")),
        P(("kv", "tp"), None),
    )
    out_specs = (P("dp", ("kv", "tp")), P(("dp", "kv"), "tp", None, None))
    shards = plain_shards
    if fits_kernel(mesh):
        shards = functools.partial(kernel_shards, mesh.shape["kv"])
    return jax.shard_map(shards, mesh=mesh, in_specs=in_specs, out_specs=out_specs, check_vma=False)
```

```python
import functools

import jax
import jax.numpy as jnp
from jax import lax
from jax.experimental import pallas as pl
from jax.experimental.pallas import tpu as pltpu
from jax.sharding import PartitionSpec as P

D = 2048


epsilon = 1e-06


def plain_shards(
    tokens,
    state,
    mix_gain,
    w_query,
    w_key,
    w_decay,
    w_value,
    w_gate,
    decay_offset,
    head_gain,
    w_out,
    mlp_gain,
    w_up,
    w_down,
):
    seq_dev = state.shape[0]
    heads_here = state.shape[1]
    key_dim = state.shape[2]
    val_dim = state.shape[3]
    weights = (w_query, w_key, w_decay, w_value, w_gate)
    tok_cols = lax.all_gather(tokens, "tp", axis=1, tiled=True)
    tok_float = tok_cols.astype(jnp.float32)
    squares = jnp.sum(tok_float * tok_float, axis=1)
    scaled = (tok_float * mix_gain).astype(jnp.bfloat16)
    kv_index = lax.axis_index("kv")
    projected = lax.psum_scatter(
        jnp.concatenate(
            [jnp.dot(scaled, weight, preferred_element_type=jnp.float32) for weight in weights],
            axis=1,
        ),
        "kv",
        scatter_dimension=0,
        tiled=True,
    )
    all_sums = lax.psum(squares, "kv")
    row_sums = lax.dynamic_slice_in_dim(all_sums, kv_index * seq_dev, seq_dev, 0)
    row_scale = lax.rsqrt(row_sums / D + epsilon)[:, None]
    projected = projected * row_scale
    key_width = heads_here * key_dim
    val_width = heads_here * val_dim
    queries = (projected[:, :key_width] * key_dim ** (-0.5)).reshape(seq_dev, heads_here, key_dim)
    new_keys = projected[:, key_width : 2 * key_width].reshape(seq_dev, heads_here, key_dim)
    retain = jax.nn.sigmoid(projected[:, 2 * key_width : 3 * key_width] + decay_offset).reshape(
        seq_dev, heads_here, key_dim
    )
    values = projected[:, 3 * key_width : 3 * key_width + val_width].reshape(
        seq_dev, heads_here, val_dim
    )
    gates = projected[:, 3 * key_width + val_width :]
    new_state = retain[..., None] * state + new_keys[..., None] * values[:, :, None, :]
    readout = jnp.einsum("bhk,bhkv->bhv", queries, new_state, precision=lax.Precision.HIGHEST)
    readout = (
        readout
        * lax.rsqrt(jnp.mean(readout * readout, axis=2, keepdims=True) + epsilon)
        * head_gain
    )
    gated = (readout.reshape(seq_dev, val_width) * jax.nn.silu(gates)).astype(jnp.bfloat16)
    branch = jnp.dot(
        lax.all_gather(gated, "kv", axis=0, tiled=True), w_out, preferred_element_type=jnp.float32
    )
    own_width = tokens.shape[1]
    branch_total = lax.psum(branch.astype(jnp.bfloat16), "tp").astype(jnp.float32)
    stream_cols = (tok_float + branch_total).astype(jnp.bfloat16)
    stream = lax.all_gather(stream_cols, "kv", axis=1, tiled=True)
    stream_own = lax.dynamic_slice_in_dim(
        stream_cols, lax.axis_index("tp") * own_width, own_width, 1
    )
    stream_float = stream.astype(jnp.float32)
    mlp_scale = lax.rsqrt(jnp.mean(stream_float * stream_float, axis=1, keepdims=True) + epsilon)
    normed = (stream_float * mlp_gain).astype(jnp.bfloat16)
    hidden = jnp.dot(normed, w_up, preferred_element_type=jnp.float32) * mlp_scale
    squared = jnp.square(jax.nn.relu(hidden)).astype(jnp.bfloat16)
    down_own = lax.psum_scatter(
        lax.dot_general(
            w_down, squared, (((0,), (1,)), ((), ())), preferred_element_type=jnp.float32
        ),
        ("kv", "tp"),
        scatter_dimension=0,
        tiled=True,
    )
    mixed = (stream_own.astype(jnp.float32) + down_own.T).astype(jnp.bfloat16)
    return (mixed, new_state)


MESH = pl.DeviceIdType.MESH
ROW_CHUNK = 64
VMEM_BYTES = 67_043_328


def pick(index, values):
    chosen = values[0]
    for at in range(1, len(values)):
        chosen = jnp.where(index == at, values[at], chosen)
    return chosen


def far_first(n_kv, kv):
    orders = [
        sorted((j for j in range(n_kv) if j != me), key=lambda j: (-abs(j - me), j)) for me in range(n_kv)
    ]
    return [pick(kv, [order[at] for order in orders]) for at in range(n_kv - 1)]


def layer_kernel(
    n_kv,
    tok_hbm,
    mix_gain_hbm,
    decay_offset_hbm,
    head_gain_hbm,
    mlp_gain_hbm,
    state_hbm,
    wq_hbm,
    wk_hbm,
    wd_hbm,
    wv_hbm,
    wg_hbm,
    w_out_hbm,
    w_up_hbm,
    w_down_hbm,
    mixed_ref,
    state_ref,
    tok_ref,
    mix_gain_ref,
    decay_offset_ref,
    head_gain_ref,
    mlp_gain_ref,
    w_qkd_ref,
    wv_ref,
    wg_ref,
    w_out_ref,
    w_up_ref,
    w_down_ref,
    w_out_other,
    w_up_other,
    w_down_other,
    tok_all,
    send_a,
    send_b,
    send_c,
    recv_a,
    recv_b,
    recv_c,
    coef,
    coef_t,
    vals,
    read,
    gated_all,
    gated_rows,
    stream_all,
    squared_ref,
    down_send,
    down_own,
    down_recv,
    load_sem,
    ready_sem,
    tok_sem,
    w_out_sem,
    proj_sem,
    gated_sem,
    stream_send_sem,
    stream_recv_sem,
    down_sem,
):
    f32, bf16 = jnp.float32, jnp.bfloat16
    kv, tp = lax.axis_index("kv"), lax.axis_index("tp")
    other = 1 - tp
    rows, half = tok_ref.shape
    seqs, heads, key_dim, val_dim = state_ref.shape
    key_width, val_width = heads * key_dim, heads * val_dim
    width = 2 * n_kv * half
    far = far_first(n_kv, kv)
    near = far[::-1]

    def remote(src, dst, send_sem, recv_sem, to_kv, to_tp):
        return pltpu.make_async_remote_copy(
            src_ref=src,
            dst_ref=dst,
            send_sem=send_sem,
            recv_sem=recv_sem,
            device_id={"kv": to_kv, "tp": to_tp},
            device_id_type=MESH,
        )

    def signal(sem, to_kv, to_tp):
        pl.semaphore_signal(sem, inc=1, device_id={"kv": to_kv, "tp": to_tp}, device_id_type=MESH)

    barrier = pltpu.get_barrier_semaphore()

    @pl.when(tp == 1)
    def _():
        signal(barrier, kv, 0)

    for j in far:
        signal(barrier, j, 1)

        @pl.when(j > kv)
        def _():
            signal(barrier, j, 0)

    loads = {}
    at_sem = {}
    for name, source, target in (
        ("tokens", tok_hbm, tok_ref),
        ("mix_gain", mix_gain_hbm, mix_gain_ref),
        ("q", wq_hbm, w_qkd_ref.at[0]),
        ("k", wk_hbm, w_qkd_ref.at[1]),
        ("d", wd_hbm, w_qkd_ref.at[2]),
        ("offset", decay_offset_hbm, decay_offset_ref),
        ("head_gain", head_gain_hbm, head_gain_ref),
        ("mlp_gain", mlp_gain_hbm, mlp_gain_ref),
        ("v", wv_hbm, wv_ref),
        ("g", wg_hbm, wg_ref),
        ("state", state_hbm, state_ref),
        ("up", w_up_hbm, w_up_ref),
        ("down", w_down_hbm, w_down_ref),
        ("out", w_out_hbm, w_out_ref),
    ):
        group = "q" if name in ("k", "d") else name
        sem = load_sem.at[at_sem.setdefault(group, len(at_sem))]
        loads[name] = pltpu.make_async_copy(source, target, sem)
        if name != "out":
            loads[name].start()
    loads["q"] = pltpu.make_async_copy(w_qkd_ref, w_qkd_ref, load_sem.at[at_sem["q"]])

    @pl.when(tp == 0)
    def _():
        pl.semaphore_wait(barrier, 1 + 2 * kv)
        signal(ready_sem, kv, 1)

    @pl.when(tp == 1)
    def _():
        loads["out"].start()
        pl.semaphore_wait(ready_sem, 1)

    loads["tokens"].wait()
    tok_copy = remote(tok_ref, tok_all.at[tp], tok_sem.at[0], tok_sem.at[1], kv, other)
    tok_copy.start()

    w_out_copy = remote(w_out_hbm, w_out_other, w_out_sem.at[0], w_out_sem.at[0], kv, 1)
    w_up_copy = remote(w_up_hbm, w_up_other, w_out_sem.at[1], w_out_sem.at[1], kv, 1)
    w_down_copy = remote(
        w_down_hbm.at[:, pl.ds(0, 2 * half)], w_down_other, w_out_sem.at[2], w_out_sem.at[2], kv, 1
    )

    @pl.when(tp == 0)
    def _():
        w_out_copy.start()

    @pl.when((tp == 0) & (kv > 0))
    def _():
        w_up_copy.start()

    tok_all[tp] = tok_ref[...]
    tok_own = tok_ref[...].astype(f32)
    squares = jnp.sum(tok_own * tok_own, axis=1, keepdims=True)
    loads["mix_gain"].wait()

    def half_rows(which):
        return pl.ds(pl.multiple_of(which * half, half), half)

    scaled_own = (tok_own * mix_gain_ref[tp]).astype(bf16)
    loads["q"].wait()
    early = [
        jnp.dot(scaled_own, w_qkd_ref[i, half_rows(tp), :], preferred_element_type=f32) for i in range(3)
    ]
    tok_copy.wait_recv()
    tok_other = tok_all[other].astype(f32)
    squares = squares + jnp.sum(tok_other * tok_other, axis=1, keepdims=True)
    scaled_other = (tok_other * mix_gain_ref[other]).astype(bf16)

    groups = ((send_a, recv_a), (send_b, recv_b), (send_c, recv_c))

    def fill(send, total, at):
        columns = total.shape[1]
        for owner in range(n_kv):
            send[owner, :, at : at + columns] = total[owner * seqs : (owner + 1) * seqs].astype(bf16)

    def project(name, weight_ref, send):
        loads[name].wait()
        total = jnp.dot(scaled_own, weight_ref[half_rows(tp), :], preferred_element_type=f32)
        fill(send, total + jnp.dot(scaled_other, weight_ref[half_rows(other), :], preferred_element_type=f32), 0)

    def proj_copy(group, j):
        send, recv = groups[group]
        return remote(send.at[j], recv.at[kv], proj_sem.at[group, 0], proj_sem.at[group, 1], j, tp)

    def proj_all(group):
        send, recv = groups[group]
        some = pl.ds(0, n_kv - 1)
        return remote(send.at[some], recv.at[some], proj_sem.at[group, 0], proj_sem.at[group, 1], kv, other)

    def send_lower(group):
        for j in far:

            @pl.when(j < kv)
            def _():
                proj_copy(group, j).start()

    def send_higher():
        order = sorted(
            ((group, at) for group in range(3) for at in range(n_kv - 1)),
            key=lambda item: item[1] * 2 + (0 if item[0] == 0 else 3),
        )
        for group, at in order:

            @pl.when(far[at] > kv)
            def _():
                proj_copy(group, far[at]).start()

    wide = jnp.broadcast_to(squares, (rows, 128))
    lane = lax.broadcasted_iota(jnp.int32, (seqs, 128), 1)
    for owner in range(n_kv):
        mine = slice(owner * seqs, (owner + 1) * seqs)
        high = wide[mine].astype(bf16).astype(f32)
        sums = jnp.where(lane < 64, high, wide[mine] - high)
        send_a[owner, :, 3 * key_width :] = sums.astype(bf16)
    late = [
        jnp.dot(scaled_other, w_qkd_ref[i, half_rows(other), :], preferred_element_type=f32) for i in range(3)
    ]
    for i in range(3):
        fill(send_a, early[i] + late[i], i * key_width)
    send_lower(0)
    project("v", wv_ref, send_b)
    send_lower(1)

    @pl.when(tp == 1)
    def _():
        pl.semaphore_wait(barrier, 2 * (n_kv - 1))
        signal(ready_sem, kv, 0)

    project("g", wg_ref, send_c)
    send_lower(2)

    @pl.when(tp == 0)
    def _():
        pl.semaphore_wait(ready_sem, 1)

    send_higher()

    def gathered(group):
        send, recv = groups[group]
        total = send[kv].astype(f32)
        proj_all(group).wait_recv()
        for j in near:
            total = total + recv[j].astype(f32)
        return total

    group_a = gathered(0)
    row_sums = group_a[:, 3 * key_width : 3 * key_width + 1] + group_a[:, 3 * key_width + 64 : 3 * key_width + 65]
    row_scale = lax.rsqrt(row_sums * (1.0 / width) + epsilon)
    queries = group_a[:, :key_width] * (row_scale * key_dim**-0.5)
    new_keys = group_a[:, key_width : 2 * key_width] * row_scale
    loads["offset"].wait()
    retain = jax.nn.sigmoid(
        group_a[:, 2 * key_width : 3 * key_width] * row_scale + decay_offset_ref[...]
    )
    query_retain = queries * retain
    overlap = queries * new_keys
    for h in range(heads):
        cols = slice(h * key_dim, (h + 1) * key_dim)
        coef[(3 * h) * seqs : (3 * h + 1) * seqs, :] = query_retain[:, cols]
        coef[(3 * h + 1) * seqs : (3 * h + 2) * seqs, :] = new_keys[:, cols]
        coef[(3 * h + 2) * seqs : (3 * h + 3) * seqs, :] = retain[:, cols]
    coef_t[...] = coef[...].T
    loads["state"].wait()
    for h in range(heads):
        for b in range(seqs):
            at = 3 * h * seqs + b
            total = jnp.zeros((8, val_dim), f32)
            for start in range(0, key_dim, ROW_CHUNK):
                piece = slice(start, start + ROW_CHUNK)
                product = coef_t[piece, at : at + 1] * state_ref[b, h, piece, :]
                total = total + jnp.sum(product.reshape(ROW_CHUNK // 8, 8, val_dim), axis=0)
            read[h, b : b + 1, :] = jnp.sum(total, axis=0, keepdims=True)

    values = gathered(1) * row_scale
    vals[...] = values
    gates = gathered(2) * row_scale
    loads["head_gain"].wait()
    for h in range(heads):
        cols = slice(h * val_dim, (h + 1) * val_dim)
        dots = jnp.sum(overlap[:, h * key_dim : (h + 1) * key_dim], axis=1, keepdims=True)
        readout = read[h] + dots * values[:, cols]
        mean = jnp.mean(readout * readout, axis=1, keepdims=True)
        gate = gates[:, cols]
        gated_all[tp, kv, :, cols] = (
            readout * lax.rsqrt(mean + epsilon) * head_gain_ref[...] * (gate * jax.nn.sigmoid(gate))
        ).astype(bf16)

    def gated_copy(j):
        block = gated_all.at[tp, kv]
        return remote(block, block, gated_sem.at[0], gated_sem.at[1 + tp], j, 1)

    def gated_some(from_tp, count):
        blocks = gated_all.at[from_tp, pl.ds(0, count)]
        return remote(blocks, blocks, gated_sem.at[0], gated_sem.at[1 + from_tp], kv, other)

    for j in far:
        gated_copy(j).start()

    @pl.when(tp == 0)
    def _():
        gated_copy(kv).start()

    @pl.when((tp == 0) & (kv > 0))
    def _():
        w_down_copy.start()

    for h in range(heads):
        for b in range(seqs):
            at = 3 * h * seqs + b
            value_row = vals[b : b + 1, h * val_dim : (h + 1) * val_dim]
            for start in range(0, key_dim, ROW_CHUNK):
                piece = slice(start, start + ROW_CHUNK)
                state_ref[b, h, piece, :] = (
                    coef_t[piece, at + 2 * seqs : at + 2 * seqs + 1] * state_ref[b, h, piece, :]
                    + coef_t[piece, at + seqs : at + seqs + 1] * value_row
                )

    tok_copy.wait_send()
    for group in range(3):
        proj_all(group).wait_send()

    def stream_copy(j, to_tp, owner):
        block = stream_all.at[owner]
        return remote(block, block, stream_send_sem.at[to_tp], stream_recv_sem.at[owner], j, to_tp)

    def out_rows(from_tp):
        for owner in range(n_kv):
            gated_rows[owner * seqs : (owner + 1) * seqs, :] = gated_all[from_tp, owner].astype(f32)
        return gated_rows[...].astype(bf16)

    @pl.when(tp == 1)
    def _():
        gated_some(1, n_kv - 1).wait_recv()
        loads["out"].wait()
        branch = jnp.dot(out_rows(1), w_out_ref[...], preferred_element_type=f32)
        w_out_copy.wait_recv()
        gated_some(0, n_kv).wait_recv()
        branch = branch + jnp.dot(out_rows(0), w_out_other[...], preferred_element_type=f32)
        for i in range(2):
            stream_all[kv, i] = (tok_all[i].astype(f32) + branch[:, i * half : (i + 1) * half]).astype(bf16)
        for to_tp in (1, 0):
            for j in far:
                stream_copy(j, to_tp, kv).start()
        stream_copy(kv, 0, kv).start()

        gated_some(1, n_kv - 1).wait_send()

    loads["mlp_gain"].wait()
    loads["up"].wait()

    @pl.when(tp == 0)
    def _():
        gated_some(0, n_kv).wait_send()
        w_out_copy.wait_send()

        @pl.when(kv > 0)
        def _():
            w_up_copy.wait_send()
            w_down_copy.wait_send()

        stream_copy(kv, 0, kv).wait_recv()

    def hidden_units(weights_of, waits):
        hidden = [None] * len(weights_of)
        sums = None
        for step, owner in enumerate([kv] + near):
            for wait in waits[step]:
                wait()
            if step > 0:
                stream_copy(kv, tp, owner).wait_recv()
            pieces = [stream_all[owner, i].astype(f32) for i in range(2)]
            normed = jnp.concatenate(
                [(piece * mlp_gain_ref[owner, i]).astype(bf16) for i, piece in enumerate(pieces)], axis=1
            )
            first = pl.multiple_of(owner * (2 * half), 2 * half)
            for at, ref in enumerate(weights_of):
                term = jnp.dot(normed, ref[pl.ds(first, 2 * half), :], preferred_element_type=f32)
                hidden[at] = term if step == 0 else hidden[at] + term
            part = sum(jnp.sum(piece * piece, axis=1, keepdims=True) for piece in pieces)
            sums = part if sums is None else sums + part
        mlp_scale = lax.rsqrt(sums * (1.0 / width) + epsilon)
        active = [jnp.maximum(units * mlp_scale, 0.0) for units in hidden]
        squared = [(units * units).astype(bf16) for units in active]
        squared_ref[...] = squared[0]
        return squared

    serves = (tp == 1) & (kv > 0)

    def down_copy(at, j, to_tp):
        return remote(down_send.at[at, to_tp], down_recv.at[2 * kv + tp], down_sem.at[0], down_sem.at[1], j, to_tp)

    def down_columns(first, columns):
        return jnp.dot(
            squared_ref[...],
            w_down_ref[:, pl.ds(pl.multiple_of(first, half), columns)],
            preferred_element_type=f32,
        )

    def down_chip(at, j):
        term = down_columns(2 * j * half, 2 * half)
        for i in range(2):
            down_send[at, i] = term[:, i * half : (i + 1) * half].astype(bf16)
            down_copy(at, j, i).start()

    def down_pair():
        term = down_columns(2 * kv * half, 2 * half)
        for i in range(2):
            down_own[i] = term[:, i * half : (i + 1) * half]
            down_send[n_kv - 1, i] = term[:, i * half : (i + 1) * half].astype(bf16)
        down_copy(n_kv - 1, kv, other).start()

    @pl.when(serves)
    def _():
        waits = [[w_up_copy.wait_recv], [loads["down"].wait, w_down_copy.wait_recv]] + [[]] * (n_kv - 2)
        squared = hidden_units((w_up_ref, w_up_other), waits)
        for i in range(2):
            cols = slice(i * half, (i + 1) * half)
            term = jnp.dot(squared[0], w_down_ref[:, cols], preferred_element_type=f32)
            term = term + jnp.dot(squared[1], w_down_other[:, cols], preferred_element_type=f32)
            down_send[0, i] = term.astype(bf16)
            down_copy(0, 0, i).start()

    @pl.when(jnp.logical_not(serves))
    def _():
        hidden_units((w_up_ref,), [[], [loads["down"].wait]] + [[]] * (n_kv - 2))

    @pl.when(kv == 0)
    def _():
        down_pair()
        for j in range(n_kv - 1, 0, -1):
            down_chip(j - 1, j)

    @pl.when(kv > 0)
    def _():
        orders = [
            sorted((j for j in range(1, n_kv) if j != me), key=lambda j: (-abs(j - me), j)) for me in range(n_kv)
        ]
        for at in range(n_kv - 2):
            down_chip(at + 1, pick(kv, [order[at] for order in orders]))
        down_pair()


    @pl.when(tp == 1)
    def _():
        remote(stream_all, stream_all, stream_send_sem.at[0], stream_recv_sem.at[0], kv, 0).wait_send()
        some = stream_all.at[pl.ds(0, n_kv - 1)]
        remote(some, some, stream_send_sem.at[1], stream_recv_sem.at[0], kv, 0).wait_send()

    def down_blocks(count):
        some = down_recv.at[pl.ds(0, count)]
        return remote(some, some, down_sem.at[0], down_sem.at[1], kv, other)

    def finish(count, slots):
        total = stream_all[kv, tp].astype(f32) + down_own[tp]
        down_blocks(count).wait_recv()
        for slot in slots:
            total = total + down_recv[slot].astype(f32)
        mixed_ref[...] = total.astype(bf16)

    @pl.when(kv == 0)
    def _():
        finish(n_kv, [other] + [2 * j + 1 for j in range(1, n_kv)])

    @pl.when(kv > 0)
    def _():
        finish(2 * n_kv - 1, [2 * kv + other] + [2 * j + i for j in near for i in range(2)])

    @pl.when((kv == 0) | (tp == 1))
    def _():
        down_blocks(2 * n_kv - 1).wait_send()

    @pl.when((kv > 0) & (tp == 0))
    def _():
        down_blocks(2 * n_kv - 3).wait_send()


def write_kernel(mixed_ref, state_ref, mixed_hbm, state_hbm, state_sem, mixed_sem):
    seqs, heads = state_ref.shape[:2]
    copies = [pltpu.make_async_copy(mixed_ref, mixed_hbm, mixed_sem.at[0])]
    for b in range(seqs):
        for h in range(heads):
            copies.append(
                pltpu.make_async_copy(state_ref.at[b, h], state_hbm.at[b, h], state_sem.at[b, h])
            )
    for copy in copies:
        copy.start()
    for copy in copies:
        copy.wait()


def kernel_shards(
    n_kv,
    tokens,
    state,
    mix_gain,
    w_query,
    w_key,
    w_decay,
    w_value,
    w_gate,
    decay_offset,
    head_gain,
    w_out,
    mlp_gain,
    w_up,
    w_down,
):
    f32, bf16 = jnp.float32, jnp.bfloat16
    rows, half = tokens.shape
    seqs, heads, key_dim, val_dim = state.shape
    key_width, val_width = heads * key_dim, heads * val_dim
    vmem = pl.BlockSpec(memory_space=pltpu.VMEM)
    hbm = pl.BlockSpec(memory_space=pltpu.HBM)
    weights = (w_query, w_key, w_decay, w_value, w_gate, w_out, w_up, w_down)
    a_width = 3 * key_width + 128
    coef_rows = 3 * heads * seqs
    coef_rows += -coef_rows % 8
    dma = pltpu.SemaphoreType.DMA
    scratch = (
        [
            pltpu.VMEM(tokens.shape, bf16),
            pltpu.VMEM((2, 1, half), f32),
            pltpu.VMEM((1, key_width), f32),
            pltpu.VMEM((1, val_dim), f32),
            pltpu.VMEM((n_kv, 2, 1, half), f32),
        ]
        + [pltpu.VMEM((3,) + w_query.shape, bf16)]
        + [pltpu.VMEM(weight.shape, bf16) for weight in weights[3:]]
        + [
            pltpu.VMEM(w_out.shape, bf16),
            pltpu.VMEM(w_up.shape, bf16),
            pltpu.VMEM((w_down.shape[0], 2 * half), bf16),
            pltpu.VMEM((2, rows, half), bf16),
            pltpu.VMEM((n_kv, seqs, a_width), bf16),
            pltpu.VMEM((n_kv, seqs, val_width), bf16),
            pltpu.VMEM((n_kv, seqs, val_width), bf16),
            pltpu.VMEM((n_kv, seqs, a_width), bf16),
            pltpu.VMEM((n_kv, seqs, val_width), bf16),
            pltpu.VMEM((n_kv, seqs, val_width), bf16),
            pltpu.VMEM((coef_rows, key_dim), f32),
            pltpu.VMEM((key_dim, coef_rows), f32),
            pltpu.VMEM((seqs, val_width), f32),
            pltpu.VMEM((heads, seqs, val_dim), f32),
            pltpu.VMEM((2, n_kv, seqs, val_width), bf16),
            pltpu.VMEM((rows, val_width), f32),
            pltpu.VMEM((n_kv, 2, rows, half), bf16),
            pltpu.VMEM((rows, w_up.shape[1]), bf16),
            pltpu.VMEM((n_kv, 2, rows, half), bf16),
            pltpu.VMEM((2, rows, half), f32),
            pltpu.VMEM((2 * n_kv, rows, half), bf16),
            dma((12,)),
            pltpu.SemaphoreType.REGULAR,
            dma((2,)),
            dma((3,)),
            dma((3, 2)),
            dma((3,)),
            dma((2,)),
            dma((n_kv,)),
            dma((2,)),
        ]
    )
    mixed, new_state = pl.pallas_call(
        functools.partial(layer_kernel, n_kv),
        out_shape=(
            pltpu.VMEM(tokens.shape, bf16),
            pltpu.VMEM(state.shape, f32),
        ),
        in_specs=[hbm] * 14,
        out_specs=(vmem, vmem),
        scratch_shapes=scratch,
        compiler_params=pltpu.CompilerParams(
            collective_id=0, has_side_effects=True, vmem_limit_bytes=VMEM_BYTES - 4 * state.size - 2**19
        ),
    )(
        tokens,
        mix_gain.reshape(2, 1, half),
        decay_offset.reshape(1, key_width),
        head_gain.reshape(1, val_dim),
        mlp_gain.reshape(n_kv, 2, 1, half),
        state,
        *weights,
    )
    return pl.pallas_call(
        write_kernel,
        out_shape=(
            jax.ShapeDtypeStruct(tokens.shape, bf16),
            jax.ShapeDtypeStruct(state.shape, f32),
        ),
        in_specs=[vmem] * 2,
        out_specs=(hbm, hbm),
        scratch_shapes=[dma((seqs, heads)), dma((1,))],
        compiler_params=pltpu.CompilerParams(vmem_limit_bytes=2**20),
    )(
        pltpu.with_memory_space_constraint(mixed, pltpu.VMEM),
        pltpu.with_memory_space_constraint(new_state, pltpu.VMEM),
    )


def fits_kernel(mesh):
    n_kv, n_tp = mesh.shape["kv"], mesh.shape["tp"]
    return n_tp == 2 and n_kv > 1 and D % (128 * n_kv * n_tp) == 0


def solution(mesh):
    in_specs = (
        P("dp", ("kv", "tp")),
        P(("dp", "kv"), "tp", None, None),
        P("kv"),
        P("kv", "tp"),
        P("kv", "tp"),
        P("kv", "tp"),
        P("kv", "tp"),
        P("kv", "tp"),
        P("tp"),
        P(),
        P("tp", "kv"),
        P(),
        P(None, ("kv", "tp")),
        P(("kv", "tp"), None),
    )
    out_specs = (P("dp", ("kv", "tp")), P(("dp", "kv"), "tp", None, None))
    shards = plain_shards
    if fits_kernel(mesh):
        shards = functools.partial(kernel_shards, mesh.shape["kv"])
    return jax.shard_map(shards, mesh=mesh, in_specs=in_specs, out_specs=out_specs, check_vma=False)
```

```python
import functools

import jax
import jax.numpy as jnp
from jax import lax
from jax.experimental import pallas as pl
from jax.experimental.pallas import tpu as pltpu
from jax.sharding import PartitionSpec as P

D = 2048


epsilon = 1e-06


def plain_shards(
    tokens,
    state,
    mix_gain,
    w_query,
    w_key,
    w_decay,
    w_value,
    w_gate,
    decay_offset,
    head_gain,
    w_out,
    mlp_gain,
    w_up,
    w_down,
):
    seq_dev = state.shape[0]
    heads_here = state.shape[1]
    key_dim = state.shape[2]
    val_dim = state.shape[3]
    weights = (w_query, w_key, w_decay, w_value, w_gate)
    tok_cols = lax.all_gather(tokens, "tp", axis=1, tiled=True)
    tok_float = tok_cols.astype(jnp.float32)
    squares = jnp.sum(tok_float * tok_float, axis=1)
    scaled = (tok_float * mix_gain).astype(jnp.bfloat16)
    kv_index = lax.axis_index("kv")
    projected = lax.psum_scatter(
        jnp.concatenate(
            [jnp.dot(scaled, weight, preferred_element_type=jnp.float32) for weight in weights],
            axis=1,
        ),
        "kv",
        scatter_dimension=0,
        tiled=True,
    )
    all_sums = lax.psum(squares, "kv")
    row_sums = lax.dynamic_slice_in_dim(all_sums, kv_index * seq_dev, seq_dev, 0)
    row_scale = lax.rsqrt(row_sums / D + epsilon)[:, None]
    projected = projected * row_scale
    key_width = heads_here * key_dim
    val_width = heads_here * val_dim
    queries = (projected[:, :key_width] * key_dim ** (-0.5)).reshape(seq_dev, heads_here, key_dim)
    new_keys = projected[:, key_width : 2 * key_width].reshape(seq_dev, heads_here, key_dim)
    retain = jax.nn.sigmoid(projected[:, 2 * key_width : 3 * key_width] + decay_offset).reshape(
        seq_dev, heads_here, key_dim
    )
    values = projected[:, 3 * key_width : 3 * key_width + val_width].reshape(
        seq_dev, heads_here, val_dim
    )
    gates = projected[:, 3 * key_width + val_width :]
    new_state = retain[..., None] * state + new_keys[..., None] * values[:, :, None, :]
    readout = jnp.einsum("bhk,bhkv->bhv", queries, new_state, precision=lax.Precision.HIGHEST)
    readout = (
        readout
        * lax.rsqrt(jnp.mean(readout * readout, axis=2, keepdims=True) + epsilon)
        * head_gain
    )
    gated = (readout.reshape(seq_dev, val_width) * jax.nn.silu(gates)).astype(jnp.bfloat16)
    branch = jnp.dot(
        lax.all_gather(gated, "kv", axis=0, tiled=True), w_out, preferred_element_type=jnp.float32
    )
    own_width = tokens.shape[1]
    branch_total = lax.psum(branch.astype(jnp.bfloat16), "tp").astype(jnp.float32)
    stream_cols = (tok_float + branch_total).astype(jnp.bfloat16)
    stream = lax.all_gather(stream_cols, "kv", axis=1, tiled=True)
    stream_own = lax.dynamic_slice_in_dim(
        stream_cols, lax.axis_index("tp") * own_width, own_width, 1
    )
    stream_float = stream.astype(jnp.float32)
    mlp_scale = lax.rsqrt(jnp.mean(stream_float * stream_float, axis=1, keepdims=True) + epsilon)
    normed = (stream_float * mlp_gain).astype(jnp.bfloat16)
    hidden = jnp.dot(normed, w_up, preferred_element_type=jnp.float32) * mlp_scale
    squared = jnp.square(jax.nn.relu(hidden)).astype(jnp.bfloat16)
    down_own = lax.psum_scatter(
        lax.dot_general(
            w_down, squared, (((0,), (1,)), ((), ())), preferred_element_type=jnp.float32
        ),
        ("kv", "tp"),
        scatter_dimension=0,
        tiled=True,
    )
    mixed = (stream_own.astype(jnp.float32) + down_own.T).astype(jnp.bfloat16)
    return (mixed, new_state)


MESH = pl.DeviceIdType.MESH
ROW_CHUNK = 64
VMEM_BYTES = 67_043_328


def pick(index, values):
    chosen = values[0]
    for at in range(1, len(values)):
        chosen = jnp.where(index == at, values[at], chosen)
    return chosen


def far_first(n_kv, kv):
    orders = [
        sorted((j for j in range(n_kv) if j != me), key=lambda j: (-abs(j - me), j)) for me in range(n_kv)
    ]
    return [pick(kv, [order[at] for order in orders]) for at in range(n_kv - 1)]


def layer_kernel(
    n_kv,
    tok_hbm,
    mix_gain_hbm,
    decay_offset_hbm,
    head_gain_hbm,
    mlp_gain_hbm,
    state_hbm,
    wq_hbm,
    wk_hbm,
    wd_hbm,
    wv_hbm,
    wg_hbm,
    w_out_hbm,
    w_up_hbm,
    w_down_hbm,
    mixed_ref,
    state_ref,
    tok_ref,
    mix_gain_ref,
    decay_offset_ref,
    head_gain_ref,
    mlp_gain_ref,
    w_qkd_ref,
    wv_ref,
    wg_ref,
    w_out_ref,
    w_up_ref,
    w_down_ref,
    w_qkd_other,
    send_other,
    w_out_other,
    w_up_other,
    w_down_other,
    tok_all,
    send_a,
    send_b,
    send_c,
    recv_a,
    recv_b,
    recv_c,
    coef,
    coef_t,
    vals,
    read,
    gated_all,
    gated_rows,
    stream_all,
    squared_ref,
    down_send,
    down_own,
    down_recv,
    load_sem,
    ready_sem,
    tok_sem,
    w_out_sem,
    proj_sem,
    gated_sem,
    stream_send_sem,
    stream_recv_sem,
    down_sem,
):
    f32, bf16 = jnp.float32, jnp.bfloat16
    kv, tp = lax.axis_index("kv"), lax.axis_index("tp")
    other = 1 - tp
    rows, half = tok_ref.shape
    seqs, heads, key_dim, val_dim = state_ref.shape
    key_width, val_width = heads * key_dim, heads * val_dim
    width = 2 * n_kv * half
    far = far_first(n_kv, kv)
    near = far[::-1]

    def remote(src, dst, send_sem, recv_sem, to_kv, to_tp):
        return pltpu.make_async_remote_copy(
            src_ref=src,
            dst_ref=dst,
            send_sem=send_sem,
            recv_sem=recv_sem,
            device_id={"kv": to_kv, "tp": to_tp},
            device_id_type=MESH,
        )

    def signal(sem, to_kv, to_tp):
        pl.semaphore_signal(sem, inc=1, device_id={"kv": to_kv, "tp": to_tp}, device_id_type=MESH)

    barrier = pltpu.get_barrier_semaphore()

    @pl.when(tp == 1)
    def _():
        signal(barrier, kv, 0)

    for j in far:
        signal(barrier, j, 1)

    loads = {}
    at_sem = {}
    for name, source, target in (
        ("tokens", tok_hbm, tok_ref),
        ("mix_gain", mix_gain_hbm, mix_gain_ref),
        ("q", wq_hbm, w_qkd_ref.at[0]),
        ("k", wk_hbm, w_qkd_ref.at[1]),
        ("d", wd_hbm, w_qkd_ref.at[2]),
        ("offset", decay_offset_hbm, decay_offset_ref),
        ("head_gain", head_gain_hbm, head_gain_ref),
        ("mlp_gain", mlp_gain_hbm, mlp_gain_ref),
        ("v", wv_hbm, wv_ref),
        ("g", wg_hbm, wg_ref),
        ("state", state_hbm, state_ref),
        ("up", w_up_hbm, w_up_ref),
        ("down", w_down_hbm, w_down_ref),
        ("out", w_out_hbm, w_out_ref),
    ):
        group = "q" if name in ("k", "d") else name
        sem = load_sem.at[at_sem.setdefault(group, len(at_sem))]
        loads[name] = pltpu.make_async_copy(source, target, sem)
        if name != "out":
            loads[name].start()
    loads["q"] = pltpu.make_async_copy(w_qkd_ref, w_qkd_ref, load_sem.at[at_sem["q"]])

    @pl.when(tp == 0)
    def _():
        pl.semaphore_wait(barrier, 1)
        signal(ready_sem, kv, 1)

    @pl.when(tp == 1)
    def _():
        loads["out"].start()
        pl.semaphore_wait(ready_sem, 1)

    loads["tokens"].wait()
    tok_copy = remote(tok_ref, tok_all.at[tp], tok_sem.at[0], tok_sem.at[1], kv, other)
    tok_copy.start()

    w_out_copy = remote(w_out_hbm, w_out_other, w_out_sem.at[0], w_out_sem.at[0], kv, 1)
    w_up_copy = remote(w_up_hbm, w_up_other, w_out_sem.at[1], w_out_sem.at[1], kv, 1)
    w_down_copy = remote(
        w_down_hbm.at[:, pl.ds(0, 2 * half)], w_down_other, w_out_sem.at[2], w_out_sem.at[2], kv, 1
    )

    qkd_copies = [
        remote(source, w_qkd_other.at[i], w_out_sem.at[1], w_out_sem.at[1], kv, 1)
        for i, source in enumerate((wq_hbm, wk_hbm, wd_hbm))
    ]
    qkd_all = remote(w_qkd_other, w_qkd_other, w_out_sem.at[1], w_out_sem.at[1], kv, 1)
    upper = kv * 2 >= n_kv
    takes_over = (tp == 1) & (kv == 0)
    hands_over = (tp == 0) & (kv == 0)

    @pl.when(hands_over)
    def _():
        for copy in qkd_copies:
            copy.start()

    @pl.when(tp == 0)
    def _():
        w_out_copy.start()

    @pl.when((tp == 0) & (kv > 0))
    def _():
        w_up_copy.start()


    def group_is_here():
        pl.semaphore_wait(barrier, 2 * (n_kv - 1))
        signal(ready_sem, kv, 0)

    @pl.when((tp == 1) & upper)
    def _():
        group_is_here()

    tok_all[tp] = tok_ref[...]
    tok_own = tok_ref[...].astype(f32)
    squares = jnp.sum(tok_own * tok_own, axis=1, keepdims=True)
    loads["mix_gain"].wait()

    def half_rows(which):
        return pl.ds(pl.multiple_of(which * half, half), half)

    scaled_own = (tok_own * mix_gain_ref[tp]).astype(bf16)
    loads["q"].wait()
    early = [
        jnp.dot(scaled_own, w_qkd_ref[i, half_rows(tp), :], preferred_element_type=f32) for i in range(3)
    ]
    tok_copy.wait_recv()
    tok_other = tok_all[other].astype(f32)
    squares = squares + jnp.sum(tok_other * tok_other, axis=1, keepdims=True)
    scaled_other = (tok_other * mix_gain_ref[other]).astype(bf16)

    groups = ((send_a, recv_a), (send_b, recv_b), (send_c, recv_c))

    def fill(send, total, at):
        columns = total.shape[1]
        for owner in range(n_kv):
            send[owner, :, at : at + columns] = total[owner * seqs : (owner + 1) * seqs].astype(bf16)

    def project(name, weight_ref, send):
        loads[name].wait()
        total = jnp.dot(scaled_own, weight_ref[half_rows(tp), :], preferred_element_type=f32)
        fill(send, total + jnp.dot(scaled_other, weight_ref[half_rows(other), :], preferred_element_type=f32), 0)

    def proj_copy(group, j):
        send, recv = groups[group]
        return remote(send.at[j], recv.at[kv], proj_sem.at[group, 0], proj_sem.at[group, 1], j, tp)

    def proj_all(group):
        send, recv = groups[group]
        some = pl.ds(0, n_kv - 1)
        return remote(send.at[some], recv.at[some], proj_sem.at[group, 0], proj_sem.at[group, 1], kv, other)

    def send_early(group):
        for j in far:

            @pl.when(upper & (j != kv - 1))
            def _():
                proj_copy(group, j).start()

    def send_late():
        order = sorted(
            ((group, at) for group in range(3) for at in range(n_kv - 1)),
            key=lambda item: item[1] * 2 + (0 if item[0] == 0 else 3),
        )
        for group, at in order:
            sends = jnp.logical_not(upper)
            if group == 0:
                sends = sends & jnp.logical_not(hands_over)

            @pl.when(sends)
            def _():
                proj_copy(group, far[at]).start()

    wide = jnp.broadcast_to(squares, (rows, 128))
    lane = lax.broadcasted_iota(jnp.int32, (seqs, 128), 1)
    for owner in range(n_kv):
        mine = slice(owner * seqs, (owner + 1) * seqs)
        high = wide[mine].astype(bf16).astype(f32)
        sums = jnp.where(lane < 64, high, wide[mine] - high)
        send_a[owner, :, 3 * key_width :] = sums.astype(bf16)
    late = [
        jnp.dot(scaled_other, w_qkd_ref[i, half_rows(other), :], preferred_element_type=f32) for i in range(3)
    ]
    for i in range(3):
        fill(send_a, early[i] + late[i], i * key_width)

    @pl.when((tp == 0) & upper)
    def _():
        pl.semaphore_wait(ready_sem, 1)

    send_early(0)
    project("v", wv_ref, send_b)
    send_early(1)

    def other_copy(j):
        return remote(send_other.at[j], recv_a.at[0], w_out_sem.at[2], proj_sem.at[0, 1], j, 0)

    @pl.when(takes_over)
    def _():
        qkd_all.wait_recv()
        for owner in range(n_kv):
            send_other[owner, :, 3 * key_width :] = send_a[owner, :, 3 * key_width :]
        total = [
            jnp.dot(scaled_own, w_qkd_other[i, half_rows(tp), :], preferred_element_type=f32)
            + jnp.dot(scaled_other, w_qkd_other[i, half_rows(other), :], preferred_element_type=f32)
            for i in range(3)
        ]
        for i in range(3):
            fill(send_other, total[i], i * key_width)

    @pl.when((tp == 1) & jnp.logical_not(upper))
    def _():
        group_is_here()

    @pl.when(takes_over)
    def _():
        for j in range(n_kv - 1, 0, -1):
            other_copy(j).start()

    project("g", wg_ref, send_c)
    send_early(2)

    @pl.when(upper)
    def _():
        for group in range(3):
            proj_copy(group, kv - 1).start()


    @pl.when((tp == 0) & jnp.logical_not(upper))
    def _():
        pl.semaphore_wait(ready_sem, 1)

    send_late()

    def gathered(group):
        send, recv = groups[group]
        total = send[kv].astype(f32)
        proj_all(group).wait_recv()
        for j in near:
            total = total + recv[j].astype(f32)
        return total

    group_a = gathered(0)
    row_sums = group_a[:, 3 * key_width : 3 * key_width + 1] + group_a[:, 3 * key_width + 64 : 3 * key_width + 65]
    row_scale = lax.rsqrt(row_sums * (1.0 / width) + epsilon)
    queries = group_a[:, :key_width] * (row_scale * key_dim**-0.5)
    new_keys = group_a[:, key_width : 2 * key_width] * row_scale
    loads["offset"].wait()
    retain = jax.nn.sigmoid(
        group_a[:, 2 * key_width : 3 * key_width] * row_scale + decay_offset_ref[...]
    )
    query_retain = queries * retain
    overlap = queries * new_keys
    for h in range(heads):
        cols = slice(h * key_dim, (h + 1) * key_dim)
        coef[(3 * h) * seqs : (3 * h + 1) * seqs, :] = query_retain[:, cols]
        coef[(3 * h + 1) * seqs : (3 * h + 2) * seqs, :] = new_keys[:, cols]
        coef[(3 * h + 2) * seqs : (3 * h + 3) * seqs, :] = retain[:, cols]
    coef_t[...] = coef[...].T
    loads["state"].wait()
    for h in range(heads):
        for b in range(seqs):
            at = 3 * h * seqs + b
            total = jnp.zeros((8, val_dim), f32)
            for start in range(0, key_dim, ROW_CHUNK):
                piece = slice(start, start + ROW_CHUNK)
                product = coef_t[piece, at : at + 1] * state_ref[b, h, piece, :]
                total = total + jnp.sum(product.reshape(ROW_CHUNK // 8, 8, val_dim), axis=0)
            read[h, b : b + 1, :] = jnp.sum(total, axis=0, keepdims=True)

    values = gathered(1) * row_scale
    vals[...] = values
    gates = gathered(2) * row_scale
    loads["head_gain"].wait()
    for h in range(heads):
        cols = slice(h * val_dim, (h + 1) * val_dim)
        dots = jnp.sum(overlap[:, h * key_dim : (h + 1) * key_dim], axis=1, keepdims=True)
        readout = read[h] + dots * values[:, cols]
        mean = jnp.mean(readout * readout, axis=1, keepdims=True)
        gate = gates[:, cols]
        gated_all[tp, kv, :, cols] = (
            readout * lax.rsqrt(mean + epsilon) * head_gain_ref[...] * (gate * jax.nn.sigmoid(gate))
        ).astype(bf16)

    def gated_copy(j):
        block = gated_all.at[tp, kv]
        return remote(block, block, gated_sem.at[0], gated_sem.at[1 + tp], j, 1)

    def gated_some(from_tp, count):
        blocks = gated_all.at[from_tp, pl.ds(0, count)]
        return remote(blocks, blocks, gated_sem.at[0], gated_sem.at[1 + from_tp], kv, other)

    for j in far:
        gated_copy(j).start()

    @pl.when(tp == 0)
    def _():
        gated_copy(kv).start()

    @pl.when((tp == 0) & (kv > 0))
    def _():
        w_down_copy.start()

    for h in range(heads):
        for b in range(seqs):
            at = 3 * h * seqs + b
            value_row = vals[b : b + 1, h * val_dim : (h + 1) * val_dim]
            for start in range(0, key_dim, ROW_CHUNK):
                piece = slice(start, start + ROW_CHUNK)
                state_ref[b, h, piece, :] = (
                    coef_t[piece, at + 2 * seqs : at + 2 * seqs + 1] * state_ref[b, h, piece, :]
                    + coef_t[piece, at + seqs : at + seqs + 1] * value_row
                )

    tok_copy.wait_send()

    @pl.when(jnp.logical_not(hands_over))
    def _():
        proj_all(0).wait_send()

    for group in (1, 2):
        proj_all(group).wait_send()

    @pl.when(takes_over)
    def _():
        some = send_other.at[pl.ds(0, n_kv - 1)]
        remote(some, some, w_out_sem.at[2], w_out_sem.at[2], kv, 0).wait_send()

    @pl.when(hands_over)
    def _():
        qkd_all.wait_send()

    def stream_copy(j, to_tp, owner):
        block = stream_all.at[owner]
        return remote(block, block, stream_send_sem.at[to_tp], stream_recv_sem.at[owner], j, to_tp)

    def out_rows(from_tp):
        for owner in range(n_kv):
            gated_rows[owner * seqs : (owner + 1) * seqs, :] = gated_all[from_tp, owner].astype(f32)
        return gated_rows[...].astype(bf16)

    @pl.when(tp == 1)
    def _():
        gated_some(1, n_kv - 1).wait_recv()
        loads["out"].wait()
        branch = jnp.dot(out_rows(1), w_out_ref[...], preferred_element_type=f32)
        w_out_copy.wait_recv()
        gated_some(0, n_kv).wait_recv()
        branch = branch + jnp.dot(out_rows(0), w_out_other[...], preferred_element_type=f32)
        for i in range(2):
            stream_all[kv, i] = (tok_all[i].astype(f32) + branch[:, i * half : (i + 1) * half]).astype(bf16)
        for to_tp in (1, 0):
            for j in far:
                stream_copy(j, to_tp, kv).start()
        stream_copy(kv, 0, kv).start()

        gated_some(1, n_kv - 1).wait_send()

    loads["mlp_gain"].wait()
    loads["up"].wait()

    @pl.when(tp == 0)
    def _():
        gated_some(0, n_kv).wait_send()
        w_out_copy.wait_send()

        @pl.when(kv > 0)
        def _():
            w_up_copy.wait_send()
            w_down_copy.wait_send()

        stream_copy(kv, 0, kv).wait_recv()

    def hidden_units(weights_of, waits):
        hidden = [None] * len(weights_of)
        sums = None
        for step, owner in enumerate([kv] + near):
            for wait in waits[step]:
                wait()
            if step > 0:
                stream_copy(kv, tp, owner).wait_recv()
            pieces = [stream_all[owner, i].astype(f32) for i in range(2)]
            normed = jnp.concatenate(
                [(piece * mlp_gain_ref[owner, i]).astype(bf16) for i, piece in enumerate(pieces)], axis=1
            )
            first = pl.multiple_of(owner * (2 * half), 2 * half)
            for at, ref in enumerate(weights_of):
                term = jnp.dot(normed, ref[pl.ds(first, 2 * half), :], preferred_element_type=f32)
                hidden[at] = term if step == 0 else hidden[at] + term
            part = sum(jnp.sum(piece * piece, axis=1, keepdims=True) for piece in pieces)
            sums = part if sums is None else sums + part
        mlp_scale = lax.rsqrt(sums * (1.0 / width) + epsilon)
        active = [jnp.maximum(units * mlp_scale, 0.0) for units in hidden]
        squared = [(units * units).astype(bf16) for units in active]
        squared_ref[...] = squared[0]
        return squared

    serves = (tp == 1) & (kv > 0)

    def down_copy(at, j, to_tp):
        return remote(down_send.at[at, to_tp], down_recv.at[2 * kv + tp], down_sem.at[0], down_sem.at[1], j, to_tp)

    def down_columns(first, columns):
        return jnp.dot(
            squared_ref[...],
            w_down_ref[:, pl.ds(pl.multiple_of(first, half), columns)],
            preferred_element_type=f32,
        )

    def down_chip(at, j):
        term = down_columns(2 * j * half, 2 * half)
        for i in range(2):
            down_send[at, i] = term[:, i * half : (i + 1) * half].astype(bf16)
            down_copy(at, j, i).start()

    def down_pair():
        term = down_columns(2 * kv * half, 2 * half)
        for i in range(2):
            down_own[i] = term[:, i * half : (i + 1) * half]
            down_send[n_kv - 1, i] = term[:, i * half : (i + 1) * half].astype(bf16)
        down_copy(n_kv - 1, kv, other).start()

    @pl.when(serves)
    def _():
        waits = [[w_up_copy.wait_recv], [loads["down"].wait, w_down_copy.wait_recv]] + [[]] * (n_kv - 2)
        squared = hidden_units((w_up_ref, w_up_other), waits)
        for i in range(2):
            cols = slice(i * half, (i + 1) * half)
            term = jnp.dot(squared[0], w_down_ref[:, cols], preferred_element_type=f32)
            term = term + jnp.dot(squared[1], w_down_other[:, cols], preferred_element_type=f32)
            down_send[0, i] = term.astype(bf16)
            down_copy(0, 0, i).start()

    @pl.when(jnp.logical_not(serves))
    def _():
        hidden_units((w_up_ref,), [[], [loads["down"].wait]] + [[]] * (n_kv - 2))

    @pl.when(kv == 0)
    def _():
        down_pair()
        for j in range(n_kv - 1, 0, -1):
            down_chip(j - 1, j)

    @pl.when(kv > 0)
    def _():
        orders = [
            sorted((j for j in range(1, n_kv) if j != me), key=lambda j: (-abs(j - me), j)) for me in range(n_kv)
        ]
        for at in range(n_kv - 2):
            down_chip(at + 1, pick(kv, [order[at] for order in orders]))
        down_pair()


    @pl.when(tp == 1)
    def _():
        remote(stream_all, stream_all, stream_send_sem.at[0], stream_recv_sem.at[0], kv, 0).wait_send()
        some = stream_all.at[pl.ds(0, n_kv - 1)]
        remote(some, some, stream_send_sem.at[1], stream_recv_sem.at[0], kv, 0).wait_send()

    def down_blocks(count):
        some = down_recv.at[pl.ds(0, count)]
        return remote(some, some, down_sem.at[0], down_sem.at[1], kv, other)

    def finish(count, slots):
        total = stream_all[kv, tp].astype(f32) + down_own[tp]
        down_blocks(count).wait_recv()
        for slot in slots:
            total = total + down_recv[slot].astype(f32)
        mixed_ref[...] = total.astype(bf16)

    @pl.when(kv == 0)
    def _():
        finish(n_kv, [other] + [2 * j + 1 for j in range(1, n_kv)])

    @pl.when(kv > 0)
    def _():
        finish(2 * n_kv - 1, [2 * kv + other] + [2 * j + i for j in near for i in range(2)])

    @pl.when((kv == 0) | (tp == 1))
    def _():
        down_blocks(2 * n_kv - 1).wait_send()

    @pl.when((kv > 0) & (tp == 0))
    def _():
        down_blocks(2 * n_kv - 3).wait_send()


def write_kernel(mixed_ref, state_ref, mixed_hbm, state_hbm, state_sem, mixed_sem):
    seqs, heads = state_ref.shape[:2]
    copies = [pltpu.make_async_copy(mixed_ref, mixed_hbm, mixed_sem.at[0])]
    for b in range(seqs):
        for h in range(heads):
            copies.append(
                pltpu.make_async_copy(state_ref.at[b, h], state_hbm.at[b, h], state_sem.at[b, h])
            )
    for copy in copies:
        copy.start()
    for copy in copies:
        copy.wait()


def kernel_shards(
    n_kv,
    tokens,
    state,
    mix_gain,
    w_query,
    w_key,
    w_decay,
    w_value,
    w_gate,
    decay_offset,
    head_gain,
    w_out,
    mlp_gain,
    w_up,
    w_down,
):
    f32, bf16 = jnp.float32, jnp.bfloat16
    rows, half = tokens.shape
    seqs, heads, key_dim, val_dim = state.shape
    key_width, val_width = heads * key_dim, heads * val_dim
    vmem = pl.BlockSpec(memory_space=pltpu.VMEM)
    hbm = pl.BlockSpec(memory_space=pltpu.HBM)
    weights = (w_query, w_key, w_decay, w_value, w_gate, w_out, w_up, w_down)
    a_width = 3 * key_width + 128
    coef_rows = 3 * heads * seqs
    coef_rows += -coef_rows % 8
    dma = pltpu.SemaphoreType.DMA
    scratch = (
        [
            pltpu.VMEM(tokens.shape, bf16),
            pltpu.VMEM((2, 1, half), f32),
            pltpu.VMEM((1, key_width), f32),
            pltpu.VMEM((1, val_dim), f32),
            pltpu.VMEM((n_kv, 2, 1, half), f32),
        ]
        + [pltpu.VMEM((3,) + w_query.shape, bf16)]
        + [pltpu.VMEM(weight.shape, bf16) for weight in weights[3:]]
        + [
            pltpu.VMEM((3,) + w_query.shape, bf16),
            pltpu.VMEM((n_kv, seqs, a_width), bf16),
            pltpu.VMEM(w_out.shape, bf16),
            pltpu.VMEM(w_up.shape, bf16),
            pltpu.VMEM((w_down.shape[0], 2 * half), bf16),
            pltpu.VMEM((2, rows, half), bf16),
            pltpu.VMEM((n_kv, seqs, a_width), bf16),
            pltpu.VMEM((n_kv, seqs, val_width), bf16),
            pltpu.VMEM((n_kv, seqs, val_width), bf16),
            pltpu.VMEM((n_kv, seqs, a_width), bf16),
            pltpu.VMEM((n_kv, seqs, val_width), bf16),
            pltpu.VMEM((n_kv, seqs, val_width), bf16),
            pltpu.VMEM((coef_rows, key_dim), f32),
            pltpu.VMEM((key_dim, coef_rows), f32),
            pltpu.VMEM((seqs, val_width), f32),
            pltpu.VMEM((heads, seqs, val_dim), f32),
            pltpu.VMEM((2, n_kv, seqs, val_width), bf16),
            pltpu.VMEM((rows, val_width), f32),
            pltpu.VMEM((n_kv, 2, rows, half), bf16),
            pltpu.VMEM((rows, w_up.shape[1]), bf16),
            pltpu.VMEM((n_kv, 2, rows, half), bf16),
            pltpu.VMEM((2, rows, half), f32),
            pltpu.VMEM((2 * n_kv, rows, half), bf16),
            dma((12,)),
            pltpu.SemaphoreType.REGULAR,
            dma((2,)),
            dma((3,)),
            dma((3, 2)),
            dma((3,)),
            dma((2,)),
            dma((n_kv,)),
            dma((2,)),
        ]
    )
    mixed, new_state = pl.pallas_call(
        functools.partial(layer_kernel, n_kv),
        out_shape=(
            pltpu.VMEM(tokens.shape, bf16),
            pltpu.VMEM(state.shape, f32),
        ),
        in_specs=[hbm] * 14,
        out_specs=(vmem, vmem),
        scratch_shapes=scratch,
        compiler_params=pltpu.CompilerParams(
            collective_id=0, has_side_effects=True, vmem_limit_bytes=VMEM_BYTES - 4 * state.size - 2**19
        ),
    )(
        tokens,
        mix_gain.reshape(2, 1, half),
        decay_offset.reshape(1, key_width),
        head_gain.reshape(1, val_dim),
        mlp_gain.reshape(n_kv, 2, 1, half),
        state,
        *weights,
    )
    return pl.pallas_call(
        write_kernel,
        out_shape=(
            jax.ShapeDtypeStruct(tokens.shape, bf16),
            jax.ShapeDtypeStruct(state.shape, f32),
        ),
        in_specs=[vmem] * 2,
        out_specs=(hbm, hbm),
        scratch_shapes=[dma((seqs, heads)), dma((1,))],
        compiler_params=pltpu.CompilerParams(vmem_limit_bytes=2**20),
    )(
        pltpu.with_memory_space_constraint(mixed, pltpu.VMEM),
        pltpu.with_memory_space_constraint(new_state, pltpu.VMEM),
    )


def fits_kernel(mesh):
    n_kv, n_tp = mesh.shape["kv"], mesh.shape["tp"]
    return n_tp == 2 and n_kv > 1 and D % (128 * n_kv * n_tp) == 0


def solution(mesh):
    in_specs = (
        P("dp", ("kv", "tp")),
        P(("dp", "kv"), "tp", None, None),
        P("kv"),
        P("kv", "tp"),
        P("kv", "tp"),
        P("kv", "tp"),
        P("kv", "tp"),
        P("kv", "tp"),
        P("tp"),
        P(),
        P("tp", "kv"),
        P(),
        P(None, ("kv", "tp")),
        P(("kv", "tp"), None),
    )
    out_specs = (P("dp", ("kv", "tp")), P(("dp", "kv"), "tp", None, None))
    shards = plain_shards
    if fits_kernel(mesh):
        shards = functools.partial(kernel_shards, mesh.shape["kv"])
    return jax.shard_map(shards, mesh=mesh, in_specs=in_specs, out_specs=out_specs, check_vma=False)
```

```python
import functools

import jax
import jax.numpy as jnp
from jax import lax
from jax.experimental import pallas as pl
from jax.experimental.pallas import tpu as pltpu
from jax.sharding import PartitionSpec as P

D = 2048


epsilon = 1e-06


def plain_shards(
    tokens,
    state,
    mix_gain,
    w_query,
    w_key,
    w_decay,
    w_value,
    w_gate,
    decay_offset,
    head_gain,
    w_out,
    mlp_gain,
    w_up,
    w_down,
):
    seq_dev = state.shape[0]
    heads_here = state.shape[1]
    key_dim = state.shape[2]
    val_dim = state.shape[3]
    weights = (w_query, w_key, w_decay, w_value, w_gate)
    tok_cols = lax.all_gather(tokens, "tp", axis=1, tiled=True)
    tok_float = tok_cols.astype(jnp.float32)
    squares = jnp.sum(tok_float * tok_float, axis=1)
    scaled = (tok_float * mix_gain).astype(jnp.bfloat16)
    kv_index = lax.axis_index("kv")
    projected = lax.psum_scatter(
        jnp.concatenate(
            [jnp.dot(scaled, weight, preferred_element_type=jnp.float32) for weight in weights],
            axis=1,
        ),
        "kv",
        scatter_dimension=0,
        tiled=True,
    )
    all_sums = lax.psum(squares, "kv")
    row_sums = lax.dynamic_slice_in_dim(all_sums, kv_index * seq_dev, seq_dev, 0)
    row_scale = lax.rsqrt(row_sums / D + epsilon)[:, None]
    projected = projected * row_scale
    key_width = heads_here * key_dim
    val_width = heads_here * val_dim
    queries = (projected[:, :key_width] * key_dim ** (-0.5)).reshape(seq_dev, heads_here, key_dim)
    new_keys = projected[:, key_width : 2 * key_width].reshape(seq_dev, heads_here, key_dim)
    retain = jax.nn.sigmoid(projected[:, 2 * key_width : 3 * key_width] + decay_offset).reshape(
        seq_dev, heads_here, key_dim
    )
    values = projected[:, 3 * key_width : 3 * key_width + val_width].reshape(
        seq_dev, heads_here, val_dim
    )
    gates = projected[:, 3 * key_width + val_width :]
    new_state = retain[..., None] * state + new_keys[..., None] * values[:, :, None, :]
    readout = jnp.einsum("bhk,bhkv->bhv", queries, new_state, precision=lax.Precision.HIGHEST)
    readout = (
        readout
        * lax.rsqrt(jnp.mean(readout * readout, axis=2, keepdims=True) + epsilon)
        * head_gain
    )
    gated = (readout.reshape(seq_dev, val_width) * jax.nn.silu(gates)).astype(jnp.bfloat16)
    branch = jnp.dot(
        lax.all_gather(gated, "kv", axis=0, tiled=True), w_out, preferred_element_type=jnp.float32
    )
    own_width = tokens.shape[1]
    branch_total = lax.psum(branch.astype(jnp.bfloat16), "tp").astype(jnp.float32)
    stream_cols = (tok_float + branch_total).astype(jnp.bfloat16)
    stream = lax.all_gather(stream_cols, "kv", axis=1, tiled=True)
    stream_own = lax.dynamic_slice_in_dim(
        stream_cols, lax.axis_index("tp") * own_width, own_width, 1
    )
    stream_float = stream.astype(jnp.float32)
    mlp_scale = lax.rsqrt(jnp.mean(stream_float * stream_float, axis=1, keepdims=True) + epsilon)
    normed = (stream_float * mlp_gain).astype(jnp.bfloat16)
    hidden = jnp.dot(normed, w_up, preferred_element_type=jnp.float32) * mlp_scale
    squared = jnp.square(jax.nn.relu(hidden)).astype(jnp.bfloat16)
    down_own = lax.psum_scatter(
        lax.dot_general(
            w_down, squared, (((0,), (1,)), ((), ())), preferred_element_type=jnp.float32
        ),
        ("kv", "tp"),
        scatter_dimension=0,
        tiled=True,
    )
    mixed = (stream_own.astype(jnp.float32) + down_own.T).astype(jnp.bfloat16)
    return (mixed, new_state)


MESH = pl.DeviceIdType.MESH
ROW_CHUNK = 64
VMEM_BYTES = 67_043_328


def pick(index, values):
    chosen = values[0]
    for at in range(1, len(values)):
        chosen = jnp.where(index == at, values[at], chosen)
    return chosen


def far_first(n_kv, kv):
    orders = [
        sorted((j for j in range(n_kv) if j != me), key=lambda j: (-abs(j - me), j)) for me in range(n_kv)
    ]
    return [pick(kv, [order[at] for order in orders]) for at in range(n_kv - 1)]


def layer_kernel(
    n_kv,
    tok_hbm,
    mix_gain_hbm,
    decay_offset_hbm,
    head_gain_hbm,
    mlp_gain_hbm,
    state_hbm,
    wq_hbm,
    wk_hbm,
    wd_hbm,
    wv_hbm,
    wg_hbm,
    w_out_hbm,
    w_up_hbm,
    w_down_hbm,
    mixed_ref,
    state_ref,
    tok_ref,
    mix_gain_ref,
    decay_offset_ref,
    head_gain_ref,
    mlp_gain_ref,
    w_qkd_ref,
    wv_ref,
    wg_ref,
    w_out_ref,
    w_up_ref,
    w_down_ref,
    w_qkd_other,
    send_other,
    w_out_other,
    w_up_other,
    w_down_other,
    tok_all,
    send_a,
    send_b,
    send_c,
    recv_a,
    recv_b,
    recv_c,
    coef,
    queries_t,
    update,
    coef_t,
    vals,
    read,
    gated_all,
    gated_rows,
    stream_all,
    squared_ref,
    down_send,
    down_own,
    down_recv,
    load_sem,
    ready_sem,
    tok_sem,
    w_out_sem,
    proj_sem,
    gated_sem,
    stream_send_sem,
    stream_recv_sem,
    down_sem,
):
    f32, bf16 = jnp.float32, jnp.bfloat16
    kv, tp = lax.axis_index("kv"), lax.axis_index("tp")
    other = 1 - tp
    rows, half = tok_ref.shape
    seqs, heads, key_dim, val_dim = state_ref.shape
    key_width, val_width = heads * key_dim, heads * val_dim
    width = 2 * n_kv * half
    far = far_first(n_kv, kv)
    near = far[::-1]

    def remote(src, dst, send_sem, recv_sem, to_kv, to_tp):
        return pltpu.make_async_remote_copy(
            src_ref=src,
            dst_ref=dst,
            send_sem=send_sem,
            recv_sem=recv_sem,
            device_id={"kv": to_kv, "tp": to_tp},
            device_id_type=MESH,
        )

    def signal(sem, to_kv, to_tp):
        pl.semaphore_signal(sem, inc=1, device_id={"kv": to_kv, "tp": to_tp}, device_id_type=MESH)

    barrier = pltpu.get_barrier_semaphore()

    @pl.when(tp == 1)
    def _():
        signal(barrier, kv, 0)

    for j in far:
        signal(barrier, j, 1)

    loads = {}
    at_sem = {}
    for name, source, target in (
        ("tokens", tok_hbm, tok_ref),
        ("mix_gain", mix_gain_hbm, mix_gain_ref),
        ("q", wq_hbm, w_qkd_ref.at[0]),
        ("k", wk_hbm, w_qkd_ref.at[1]),
        ("d", wd_hbm, w_qkd_ref.at[2]),
        ("offset", decay_offset_hbm, decay_offset_ref),
        ("head_gain", head_gain_hbm, head_gain_ref),
        ("mlp_gain", mlp_gain_hbm, mlp_gain_ref),
        ("v", wv_hbm, wv_ref),
        ("g", wg_hbm, wg_ref),
        ("state", state_hbm, state_ref),
        ("up", w_up_hbm, w_up_ref),
        ("down", w_down_hbm, w_down_ref),
        ("out", w_out_hbm, w_out_ref),
    ):
        group = "q" if name in ("k", "d") else name
        sem = load_sem.at[at_sem.setdefault(group, len(at_sem))]
        loads[name] = pltpu.make_async_copy(source, target, sem)
        if name != "out":
            loads[name].start()
    loads["q"] = pltpu.make_async_copy(w_qkd_ref, w_qkd_ref, load_sem.at[at_sem["q"]])

    @pl.when(tp == 0)
    def _():
        pl.semaphore_wait(barrier, 1)
        signal(ready_sem, kv, 1)

    @pl.when(tp == 1)
    def _():
        loads["out"].start()
        pl.semaphore_wait(ready_sem, 1)

    loads["tokens"].wait()
    tok_copy = remote(tok_ref, tok_all.at[tp], tok_sem.at[0], tok_sem.at[1], kv, other)
    tok_copy.start()

    w_out_copy = remote(w_out_hbm, w_out_other, w_out_sem.at[0], w_out_sem.at[0], kv, 1)
    w_up_copy = remote(w_up_hbm, w_up_other, w_out_sem.at[1], w_out_sem.at[1], kv, 1)
    w_down_copy = remote(
        w_down_hbm.at[:, pl.ds(0, 2 * half)], w_down_other, w_out_sem.at[2], w_out_sem.at[2], kv, 1
    )

    qkd_copies = [
        remote(source, w_qkd_other.at[i], w_out_sem.at[1], w_out_sem.at[1], kv, 1)
        for i, source in enumerate((wq_hbm, wk_hbm, wd_hbm))
    ]
    qkd_all = remote(w_qkd_other, w_qkd_other, w_out_sem.at[1], w_out_sem.at[1], kv, 1)
    upper = kv * 2 >= n_kv
    takes_over = (tp == 1) & (kv == 0)
    hands_over = (tp == 0) & (kv == 0)

    @pl.when(hands_over)
    def _():
        for copy in qkd_copies:
            copy.start()

    @pl.when(tp == 0)
    def _():
        w_out_copy.start()

    @pl.when((tp == 0) & (kv > 0))
    def _():
        w_up_copy.start()


    def group_is_here():
        pl.semaphore_wait(barrier, 2 * (n_kv - 1))
        signal(ready_sem, kv, 0)

    @pl.when((tp == 1) & upper)
    def _():
        group_is_here()

    tok_all[tp] = tok_ref[...]
    tok_own = tok_ref[...].astype(f32)
    squares = jnp.sum(tok_own * tok_own, axis=1, keepdims=True)
    loads["mix_gain"].wait()

    def half_rows(which):
        return pl.ds(pl.multiple_of(which * half, half), half)

    scaled_own = (tok_own * mix_gain_ref[tp]).astype(bf16)
    loads["q"].wait()
    early = [
        jnp.dot(scaled_own, w_qkd_ref[i, half_rows(tp), :], preferred_element_type=f32) for i in range(3)
    ]
    tok_copy.wait_recv()
    tok_other = tok_all[other].astype(f32)
    squares = squares + jnp.sum(tok_other * tok_other, axis=1, keepdims=True)
    scaled_other = (tok_other * mix_gain_ref[other]).astype(bf16)

    groups = ((send_a, recv_a), (send_b, recv_b), (send_c, recv_c))

    def fill(send, total, at):
        columns = total.shape[1]
        for owner in range(n_kv):
            send[owner, :, at : at + columns] = total[owner * seqs : (owner + 1) * seqs].astype(bf16)

    def project(weight_ref):
        total = jnp.dot(scaled_own, weight_ref[half_rows(tp), :], preferred_element_type=f32)
        return total + jnp.dot(scaled_other, weight_ref[half_rows(other), :], preferred_element_type=f32)

    def proj_copy(group, j):
        send, recv = groups[group]
        return remote(send.at[j], recv.at[kv], proj_sem.at[group, 0], proj_sem.at[group, 1], j, tp)

    def proj_all(group):
        send, recv = groups[group]
        some = pl.ds(0, n_kv - 1)
        return remote(send.at[some], recv.at[some], proj_sem.at[group, 0], proj_sem.at[group, 1], kv, other)

    def send_early(group):
        for j in far:

            @pl.when(upper & (j != kv - 1))
            def _():
                proj_copy(group, j).start()

    def send_late():
        order = sorted(
            ((group, at) for group in range(3) for at in range(n_kv - 1)),
            key=lambda item: item[1] * 2 + (0 if item[0] == 0 else 3),
        )
        for group, at in order:
            sends = jnp.logical_not(upper)
            if group == 0:
                sends = sends & jnp.logical_not(hands_over)

            @pl.when(sends)
            def _():
                proj_copy(group, far[at]).start()

    wide = jnp.broadcast_to(squares, (rows, 128))
    lane = lax.broadcasted_iota(jnp.int32, (seqs, 128), 1)
    for owner in range(n_kv):
        mine = slice(owner * seqs, (owner + 1) * seqs)
        high = wide[mine].astype(bf16).astype(f32)
        sums = jnp.where(lane < 64, high, wide[mine] - high)
        send_a[owner, :, 3 * key_width :] = sums.astype(bf16)
    late = [
        jnp.dot(scaled_other, w_qkd_ref[i, half_rows(other), :], preferred_element_type=f32) for i in range(3)
    ]
    for i in range(3):
        fill(send_a, early[i] + late[i], i * key_width)

    @pl.when((tp == 0) & upper)
    def _():
        pl.semaphore_wait(ready_sem, 1)

    send_early(0)
    loads["v"].wait()
    loads["g"].wait()
    total_v, total_g = project(wv_ref), project(wg_ref)
    fill(send_b, total_v, 0)
    fill(send_c, total_g, 0)
    send_early(1)
    send_early(2)

    @pl.when(upper)
    def _():
        for group in range(3):
            proj_copy(group, kv - 1).start()

    def other_copy(j):
        return remote(send_other.at[j], recv_a.at[0], w_out_sem.at[2], proj_sem.at[0, 1], j, 0)

    @pl.when(takes_over)
    def _():
        qkd_all.wait_recv()
        for owner in range(n_kv):
            send_other[owner, :, 3 * key_width :] = send_a[owner, :, 3 * key_width :]
        total = [
            jnp.dot(scaled_own, w_qkd_other[i, half_rows(tp), :], preferred_element_type=f32)
            + jnp.dot(scaled_other, w_qkd_other[i, half_rows(other), :], preferred_element_type=f32)
            for i in range(3)
        ]
        for i in range(3):
            fill(send_other, total[i], i * key_width)

    @pl.when((tp == 1) & jnp.logical_not(upper))
    def _():
        group_is_here()

    @pl.when(takes_over)
    def _():
        for j in range(n_kv - 1, 0, -1):
            other_copy(j).start()


    @pl.when((tp == 0) & jnp.logical_not(upper))
    def _():
        pl.semaphore_wait(ready_sem, 1)

    send_late()

    def gathered(group):
        send, recv = groups[group]
        total = send[kv].astype(f32)
        proj_all(group).wait_recv()
        for j in near:
            total = total + recv[j].astype(f32)
        return total

    group_a = gathered(0)
    row_sums = group_a[:, 3 * key_width : 3 * key_width + 1] + group_a[:, 3 * key_width + 64 : 3 * key_width + 65]
    row_scale = lax.rsqrt(row_sums * (1.0 / width) + epsilon)
    queries = group_a[:, :key_width] * (row_scale * key_dim**-0.5)
    new_keys = group_a[:, key_width : 2 * key_width] * row_scale
    loads["offset"].wait()
    retain = jax.nn.sigmoid(
        group_a[:, 2 * key_width : 3 * key_width] * row_scale + decay_offset_ref[...]
    )
    query_retain = queries * retain
    for h in range(heads):
        coef[h * seqs : (h + 1) * seqs, :] = query_retain[:, h * key_dim : (h + 1) * key_dim]
    queries_t[...] = coef[...].T
    loads["state"].wait()
    for h in range(heads):
        for b in range(seqs):
            at = h * seqs + b
            total = jnp.zeros((8, val_dim), f32)
            for start in range(0, key_dim, ROW_CHUNK):
                piece = slice(start, start + ROW_CHUNK)
                product = queries_t[piece, at : at + 1] * state_ref[b, h, piece, :]
                total = total + jnp.sum(product.reshape(ROW_CHUNK // 8, 8, val_dim), axis=0)
            read[h, b : b + 1, :] = jnp.sum(total, axis=0, keepdims=True)

    overlap = queries * new_keys
    all_dots = [
        jnp.sum(overlap[:, h * key_dim : (h + 1) * key_dim], axis=1, keepdims=True) for h in range(heads)
    ]
    values = gathered(1) * row_scale
    vals[...] = values
    loads["head_gain"].wait()
    normal = []
    for h in range(heads):
        cols = slice(h * val_dim, (h + 1) * val_dim)
        readout = read[h] + all_dots[h] * values[:, cols]
        mean = jnp.mean(readout * readout, axis=1, keepdims=True)
        normal.append(readout * lax.rsqrt(mean + epsilon) * head_gain_ref[...])
    gates = gathered(2) * row_scale
    for h in range(heads):
        cols = slice(h * val_dim, (h + 1) * val_dim)
        gate = gates[:, cols]
        gated_all[tp, kv, :, cols] = (normal[h] * (gate * jax.nn.sigmoid(gate))).astype(bf16)

    def gated_copy(j):
        block = gated_all.at[tp, kv]
        return remote(block, block, gated_sem.at[0], gated_sem.at[1 + tp], j, 1)

    def gated_some(from_tp, count):
        blocks = gated_all.at[from_tp, pl.ds(0, count)]
        return remote(blocks, blocks, gated_sem.at[0], gated_sem.at[1 + from_tp], kv, other)

    for j in far:
        gated_copy(j).start()

    @pl.when(tp == 0)
    def _():
        gated_copy(kv).start()

    @pl.when((tp == 0) & (kv > 0))
    def _():
        w_down_copy.start()

    for h in range(heads):
        cols = slice(h * key_dim, (h + 1) * key_dim)
        update[2 * h * seqs : (2 * h + 1) * seqs, :] = new_keys[:, cols]
        update[(2 * h + 1) * seqs : (2 * h + 2) * seqs, :] = retain[:, cols]
    coef_t[...] = update[...].T
    for h in range(heads):
        for b in range(seqs):
            at = 2 * h * seqs + b
            value_row = vals[b : b + 1, h * val_dim : (h + 1) * val_dim]
            for start in range(0, key_dim, ROW_CHUNK):
                piece = slice(start, start + ROW_CHUNK)
                state_ref[b, h, piece, :] = (
                    coef_t[piece, at + seqs : at + seqs + 1] * state_ref[b, h, piece, :]
                    + coef_t[piece, at : at + 1] * value_row
                )

    tok_copy.wait_send()

    @pl.when(jnp.logical_not(hands_over))
    def _():
        proj_all(0).wait_send()

    for group in (1, 2):
        proj_all(group).wait_send()

    @pl.when(takes_over)
    def _():
        some = send_other.at[pl.ds(0, n_kv - 1)]
        remote(some, some, w_out_sem.at[2], w_out_sem.at[2], kv, 0).wait_send()

    @pl.when(hands_over)
    def _():
        qkd_all.wait_send()

    def stream_copy(j, to_tp, owner):
        block = stream_all.at[owner]
        return remote(block, block, stream_send_sem.at[to_tp], stream_recv_sem.at[owner], j, to_tp)

    def out_rows(from_tp):
        for owner in range(n_kv):
            gated_rows[owner * seqs : (owner + 1) * seqs, :] = gated_all[from_tp, owner].astype(f32)
        return gated_rows[...].astype(bf16)

    @pl.when(tp == 1)
    def _():
        gated_some(1, n_kv - 1).wait_recv()
        loads["out"].wait()
        branch = jnp.dot(out_rows(1), w_out_ref[...], preferred_element_type=f32)
        w_out_copy.wait_recv()
        gated_some(0, n_kv).wait_recv()
        branch = branch + jnp.dot(out_rows(0), w_out_other[...], preferred_element_type=f32)
        for i in range(2):
            stream_all[kv, i] = (tok_all[i].astype(f32) + branch[:, i * half : (i + 1) * half]).astype(bf16)
        for to_tp in (1, 0):
            for j in far:
                stream_copy(j, to_tp, kv).start()
        stream_copy(kv, 0, kv).start()

        gated_some(1, n_kv - 1).wait_send()

    loads["mlp_gain"].wait()
    loads["up"].wait()

    @pl.when(tp == 0)
    def _():
        gated_some(0, n_kv).wait_send()
        w_out_copy.wait_send()

        @pl.when(kv > 0)
        def _():
            w_up_copy.wait_send()
            w_down_copy.wait_send()

        stream_copy(kv, 0, kv).wait_recv()

    def hidden_units(weights_of, waits):
        hidden = [None] * len(weights_of)
        sums = None
        for step, owner in enumerate([kv] + near):
            for wait in waits[step]:
                wait()
            if step > 0:
                stream_copy(kv, tp, owner).wait_recv()
            pieces = [stream_all[owner, i].astype(f32) for i in range(2)]
            normed = jnp.concatenate(
                [(piece * mlp_gain_ref[owner, i]).astype(bf16) for i, piece in enumerate(pieces)], axis=1
            )
            first = pl.multiple_of(owner * (2 * half), 2 * half)
            for at, ref in enumerate(weights_of):
                term = jnp.dot(normed, ref[pl.ds(first, 2 * half), :], preferred_element_type=f32)
                hidden[at] = term if step == 0 else hidden[at] + term
            part = sum(jnp.sum(piece * piece, axis=1, keepdims=True) for piece in pieces)
            sums = part if sums is None else sums + part
        mlp_scale = lax.rsqrt(sums * (1.0 / width) + epsilon)
        active = [jnp.maximum(units * mlp_scale, 0.0) for units in hidden]
        squared = [(units * units).astype(bf16) for units in active]
        squared_ref[...] = squared[0]
        return squared

    serves = (tp == 1) & (kv > 0)

    def down_copy(at, j, to_tp):
        return remote(down_send.at[at, to_tp], down_recv.at[2 * kv + tp], down_sem.at[0], down_sem.at[1], j, to_tp)

    def down_columns(first, columns):
        return jnp.dot(
            squared_ref[...],
            w_down_ref[:, pl.ds(pl.multiple_of(first, half), columns)],
            preferred_element_type=f32,
        )

    def down_chip(at, j):
        term = down_columns(2 * j * half, 2 * half)
        for i in range(2):
            down_send[at, i] = term[:, i * half : (i + 1) * half].astype(bf16)
            down_copy(at, j, i).start()

    def down_pair():
        term = down_columns(2 * kv * half, 2 * half)
        for i in range(2):
            down_own[i] = term[:, i * half : (i + 1) * half]
            down_send[n_kv - 1, i] = term[:, i * half : (i + 1) * half].astype(bf16)
        down_copy(n_kv - 1, kv, other).start()

    @pl.when(serves)
    def _():
        waits = [[w_up_copy.wait_recv], [loads["down"].wait, w_down_copy.wait_recv]] + [[]] * (n_kv - 2)
        squared = hidden_units((w_up_ref, w_up_other), waits)
        for i in range(2):
            cols = slice(i * half, (i + 1) * half)
            term = jnp.dot(squared[0], w_down_ref[:, cols], preferred_element_type=f32)
            term = term + jnp.dot(squared[1], w_down_other[:, cols], preferred_element_type=f32)
            down_send[0, i] = term.astype(bf16)
            down_copy(0, 0, i).start()

    @pl.when(jnp.logical_not(serves))
    def _():
        hidden_units((w_up_ref,), [[], [loads["down"].wait]] + [[]] * (n_kv - 2))

    @pl.when(kv == 0)
    def _():
        down_pair()
        for j in range(n_kv - 1, 0, -1):
            down_chip(j - 1, j)

    @pl.when(kv > 0)
    def _():
        orders = [
            sorted((j for j in range(1, n_kv) if j != me), key=lambda j: (-abs(j - me), j)) for me in range(n_kv)
        ]
        for at in range(n_kv - 2):
            down_chip(at + 1, pick(kv, [order[at] for order in orders]))
        down_pair()


    @pl.when(tp == 1)
    def _():
        remote(stream_all, stream_all, stream_send_sem.at[0], stream_recv_sem.at[0], kv, 0).wait_send()
        some = stream_all.at[pl.ds(0, n_kv - 1)]
        remote(some, some, stream_send_sem.at[1], stream_recv_sem.at[0], kv, 0).wait_send()

    def down_blocks(count):
        some = down_recv.at[pl.ds(0, count)]
        return remote(some, some, down_sem.at[0], down_sem.at[1], kv, other)

    def finish(count, slots):
        total = stream_all[kv, tp].astype(f32) + down_own[tp]
        down_blocks(count).wait_recv()
        for slot in slots:
            total = total + down_recv[slot].astype(f32)
        mixed_ref[...] = total.astype(bf16)

    @pl.when(kv == 0)
    def _():
        finish(n_kv, [other] + [2 * j + 1 for j in range(1, n_kv)])

    @pl.when(kv > 0)
    def _():
        finish(2 * n_kv - 1, [2 * kv + other] + [2 * j + i for j in near for i in range(2)])

    @pl.when((kv == 0) | (tp == 1))
    def _():
        down_blocks(2 * n_kv - 1).wait_send()

    @pl.when((kv > 0) & (tp == 0))
    def _():
        down_blocks(2 * n_kv - 3).wait_send()


def write_kernel(mixed_ref, state_ref, mixed_hbm, state_hbm, state_sem, mixed_sem):
    seqs, heads = state_ref.shape[:2]
    copies = [pltpu.make_async_copy(mixed_ref, mixed_hbm, mixed_sem.at[0])]
    for b in range(seqs):
        for h in range(heads):
            copies.append(
                pltpu.make_async_copy(state_ref.at[b, h], state_hbm.at[b, h], state_sem.at[b, h])
            )
    for copy in copies:
        copy.start()
    for copy in copies:
        copy.wait()


def kernel_shards(
    n_kv,
    tokens,
    state,
    mix_gain,
    w_query,
    w_key,
    w_decay,
    w_value,
    w_gate,
    decay_offset,
    head_gain,
    w_out,
    mlp_gain,
    w_up,
    w_down,
):
    f32, bf16 = jnp.float32, jnp.bfloat16
    rows, half = tokens.shape
    seqs, heads, key_dim, val_dim = state.shape
    key_width, val_width = heads * key_dim, heads * val_dim
    vmem = pl.BlockSpec(memory_space=pltpu.VMEM)
    hbm = pl.BlockSpec(memory_space=pltpu.HBM)
    weights = (w_query, w_key, w_decay, w_value, w_gate, w_out, w_up, w_down)
    a_width = 3 * key_width + 128
    dma = pltpu.SemaphoreType.DMA
    scratch = (
        [
            pltpu.VMEM(tokens.shape, bf16),
            pltpu.VMEM((2, 1, half), f32),
            pltpu.VMEM((1, key_width), f32),
            pltpu.VMEM((1, val_dim), f32),
            pltpu.VMEM((n_kv, 2, 1, half), f32),
        ]
        + [pltpu.VMEM((3,) + w_query.shape, bf16)]
        + [pltpu.VMEM(weight.shape, bf16) for weight in weights[3:]]
        + [
            pltpu.VMEM((3,) + w_query.shape, bf16),
            pltpu.VMEM((n_kv, seqs, a_width), bf16),
            pltpu.VMEM(w_out.shape, bf16),
            pltpu.VMEM(w_up.shape, bf16),
            pltpu.VMEM((w_down.shape[0], 2 * half), bf16),
            pltpu.VMEM((2, rows, half), bf16),
            pltpu.VMEM((n_kv, seqs, a_width), bf16),
            pltpu.VMEM((n_kv, seqs, val_width), bf16),
            pltpu.VMEM((n_kv, seqs, val_width), bf16),
            pltpu.VMEM((n_kv, seqs, a_width), bf16),
            pltpu.VMEM((n_kv, seqs, val_width), bf16),
            pltpu.VMEM((n_kv, seqs, val_width), bf16),
            pltpu.VMEM((heads * seqs, key_dim), f32),
            pltpu.VMEM((key_dim, heads * seqs), f32),
            pltpu.VMEM((2 * heads * seqs, key_dim), f32),
            pltpu.VMEM((key_dim, 2 * heads * seqs), f32),
            pltpu.VMEM((seqs, val_width), f32),
            pltpu.VMEM((heads, seqs, val_dim), f32),
            pltpu.VMEM((2, n_kv, seqs, val_width), bf16),
            pltpu.VMEM((rows, val_width), f32),
            pltpu.VMEM((n_kv, 2, rows, half), bf16),
            pltpu.VMEM((rows, w_up.shape[1]), bf16),
            pltpu.VMEM((n_kv, 2, rows, half), bf16),
            pltpu.VMEM((2, rows, half), f32),
            pltpu.VMEM((2 * n_kv, rows, half), bf16),
            dma((12,)),
            pltpu.SemaphoreType.REGULAR,
            dma((2,)),
            dma((3,)),
            dma((3, 2)),
            dma((3,)),
            dma((2,)),
            dma((n_kv,)),
            dma((2,)),
        ]
    )
    mixed, new_state = pl.pallas_call(
        functools.partial(layer_kernel, n_kv),
        out_shape=(
            pltpu.VMEM(tokens.shape, bf16),
            pltpu.VMEM(state.shape, f32),
        ),
        in_specs=[hbm] * 14,
        out_specs=(vmem, vmem),
        scratch_shapes=scratch,
        compiler_params=pltpu.CompilerParams(
            collective_id=0, has_side_effects=True, vmem_limit_bytes=VMEM_BYTES - 4 * state.size - 2**19
        ),
    )(
        tokens,
        mix_gain.reshape(2, 1, half),
        decay_offset.reshape(1, key_width),
        head_gain.reshape(1, val_dim),
        mlp_gain.reshape(n_kv, 2, 1, half),
        state,
        *weights,
    )
    return pl.pallas_call(
        write_kernel,
        out_shape=(
            jax.ShapeDtypeStruct(tokens.shape, bf16),
            jax.ShapeDtypeStruct(state.shape, f32),
        ),
        in_specs=[vmem] * 2,
        out_specs=(hbm, hbm),
        scratch_shapes=[dma((seqs, heads)), dma((1,))],
        compiler_params=pltpu.CompilerParams(vmem_limit_bytes=2**20),
    )(
        pltpu.with_memory_space_constraint(mixed, pltpu.VMEM),
        pltpu.with_memory_space_constraint(new_state, pltpu.VMEM),
    )


def fits_kernel(mesh):
    n_kv, n_tp = mesh.shape["kv"], mesh.shape["tp"]
    return n_tp == 2 and n_kv > 1 and D % (128 * n_kv * n_tp) == 0


def solution(mesh):
    in_specs = (
        P("dp", ("kv", "tp")),
        P(("dp", "kv"), "tp", None, None),
        P("kv"),
        P("kv", "tp"),
        P("kv", "tp"),
        P("kv", "tp"),
        P("kv", "tp"),
        P("kv", "tp"),
        P("tp"),
        P(),
        P("tp", "kv"),
        P(),
        P(None, ("kv", "tp")),
        P(("kv", "tp"), None),
    )
    out_specs = (P("dp", ("kv", "tp")), P(("dp", "kv"), "tp", None, None))
    shards = plain_shards
    if fits_kernel(mesh):
        shards = functools.partial(kernel_shards, mesh.shape["kv"])
    return jax.shard_map(shards, mesh=mesh, in_specs=in_specs, out_specs=out_specs, check_vma=False)
```

```python
import functools

import jax
import jax.numpy as jnp
from jax import lax
from jax.experimental import pallas as pl
from jax.experimental.pallas import tpu as pltpu
from jax.sharding import PartitionSpec as P

D = 2048


epsilon = 1e-06


def plain_shards(
    tokens,
    state,
    mix_gain,
    w_query,
    w_key,
    w_decay,
    w_value,
    w_gate,
    decay_offset,
    head_gain,
    w_out,
    mlp_gain,
    w_up,
    w_down,
):
    seq_dev = state.shape[0]
    heads_here = state.shape[1]
    key_dim = state.shape[2]
    val_dim = state.shape[3]
    weights = (w_query, w_key, w_decay, w_value, w_gate)
    tok_cols = lax.all_gather(tokens, "tp", axis=1, tiled=True)
    tok_float = tok_cols.astype(jnp.float32)
    squares = jnp.sum(tok_float * tok_float, axis=1)
    scaled = (tok_float * mix_gain).astype(jnp.bfloat16)
    kv_index = lax.axis_index("kv")
    projected = lax.psum_scatter(
        jnp.concatenate(
            [jnp.dot(scaled, weight, preferred_element_type=jnp.float32) for weight in weights],
            axis=1,
        ),
        "kv",
        scatter_dimension=0,
        tiled=True,
    )
    all_sums = lax.psum(squares, "kv")
    row_sums = lax.dynamic_slice_in_dim(all_sums, kv_index * seq_dev, seq_dev, 0)
    row_scale = lax.rsqrt(row_sums / D + epsilon)[:, None]
    projected = projected * row_scale
    key_width = heads_here * key_dim
    val_width = heads_here * val_dim
    queries = (projected[:, :key_width] * key_dim ** (-0.5)).reshape(seq_dev, heads_here, key_dim)
    new_keys = projected[:, key_width : 2 * key_width].reshape(seq_dev, heads_here, key_dim)
    retain = jax.nn.sigmoid(projected[:, 2 * key_width : 3 * key_width] + decay_offset).reshape(
        seq_dev, heads_here, key_dim
    )
    values = projected[:, 3 * key_width : 3 * key_width + val_width].reshape(
        seq_dev, heads_here, val_dim
    )
    gates = projected[:, 3 * key_width + val_width :]
    new_state = retain[..., None] * state + new_keys[..., None] * values[:, :, None, :]
    readout = jnp.einsum("bhk,bhkv->bhv", queries, new_state, precision=lax.Precision.HIGHEST)
    readout = (
        readout
        * lax.rsqrt(jnp.mean(readout * readout, axis=2, keepdims=True) + epsilon)
        * head_gain
    )
    gated = (readout.reshape(seq_dev, val_width) * jax.nn.silu(gates)).astype(jnp.bfloat16)
    branch = jnp.dot(
        lax.all_gather(gated, "kv", axis=0, tiled=True), w_out, preferred_element_type=jnp.float32
    )
    own_width = tokens.shape[1]
    branch_total = lax.psum(branch.astype(jnp.bfloat16), "tp").astype(jnp.float32)
    stream_cols = (tok_float + branch_total).astype(jnp.bfloat16)
    stream = lax.all_gather(stream_cols, "kv", axis=1, tiled=True)
    stream_own = lax.dynamic_slice_in_dim(
        stream_cols, lax.axis_index("tp") * own_width, own_width, 1
    )
    stream_float = stream.astype(jnp.float32)
    mlp_scale = lax.rsqrt(jnp.mean(stream_float * stream_float, axis=1, keepdims=True) + epsilon)
    normed = (stream_float * mlp_gain).astype(jnp.bfloat16)
    hidden = jnp.dot(normed, w_up, preferred_element_type=jnp.float32) * mlp_scale
    squared = jnp.square(jax.nn.relu(hidden)).astype(jnp.bfloat16)
    down_own = lax.psum_scatter(
        lax.dot_general(
            w_down, squared, (((0,), (1,)), ((), ())), preferred_element_type=jnp.float32
        ),
        ("kv", "tp"),
        scatter_dimension=0,
        tiled=True,
    )
    mixed = (stream_own.astype(jnp.float32) + down_own.T).astype(jnp.bfloat16)
    return (mixed, new_state)


MESH = pl.DeviceIdType.MESH
ROW_CHUNK = 64
VMEM_BYTES = 67_043_328


def pick(index, values):
    chosen = values[0]
    for at in range(1, len(values)):
        chosen = jnp.where(index == at, values[at], chosen)
    return chosen


def far_first(n_kv, kv):
    orders = [
        sorted((j for j in range(n_kv) if j != me), key=lambda j: (-abs(j - me), j)) for me in range(n_kv)
    ]
    return [pick(kv, [order[at] for order in orders]) for at in range(n_kv - 1)]


def layer_kernel(
    n_kv,
    tok_hbm,
    mix_gain_hbm,
    decay_offset_hbm,
    head_gain_hbm,
    mlp_gain_hbm,
    state_hbm,
    wq_hbm,
    wk_hbm,
    wd_hbm,
    wv_hbm,
    wg_hbm,
    w_out_hbm,
    w_up_hbm,
    w_down_hbm,
    mixed_ref,
    state_ref,
    tok_ref,
    mix_gain_ref,
    decay_offset_ref,
    head_gain_ref,
    mlp_gain_ref,
    w_qkd_ref,
    wv_ref,
    wg_ref,
    w_out_ref,
    w_up_ref,
    w_down_ref,
    w_qkd_other,
    send_other,
    w_out_other,
    w_up_other,
    w_down_other,
    tok_all,
    send_a,
    send_b,
    send_c,
    recv_a,
    recv_b,
    recv_c,
    coef,
    queries_t,
    update,
    coef_t,
    vals,
    read,
    gated_all,
    gated_rows,
    stream_all,
    squared_ref,
    down_send,
    down_own,
    down_recv,
    load_sem,
    ready_sem,
    tok_sem,
    w_out_sem,
    proj_sem,
    gated_sem,
    stream_send_sem,
    stream_recv_sem,
    down_sem,
):
    f32, bf16 = jnp.float32, jnp.bfloat16
    kv, tp = lax.axis_index("kv"), lax.axis_index("tp")
    other = 1 - tp
    rows, half = tok_ref.shape
    seqs, heads, key_dim, val_dim = state_ref.shape
    key_width, val_width = heads * key_dim, heads * val_dim
    width = 2 * n_kv * half
    far = far_first(n_kv, kv)
    near = far[::-1]

    def remote(src, dst, send_sem, recv_sem, to_kv, to_tp):
        return pltpu.make_async_remote_copy(
            src_ref=src,
            dst_ref=dst,
            send_sem=send_sem,
            recv_sem=recv_sem,
            device_id={"kv": to_kv, "tp": to_tp},
            device_id_type=MESH,
        )

    def signal(sem, to_kv, to_tp):
        pl.semaphore_signal(sem, inc=1, device_id={"kv": to_kv, "tp": to_tp}, device_id_type=MESH)

    barrier = pltpu.get_barrier_semaphore()

    @pl.when(tp == 1)
    def _():
        signal(barrier, kv, 0)

    for j in far:
        signal(barrier, j, 1)

    loads = {}
    at_sem = {}
    for name, source, target in (
        ("tokens", tok_hbm, tok_ref),
        ("mix_gain", mix_gain_hbm, mix_gain_ref),
        ("q", wq_hbm, w_qkd_ref.at[0]),
        ("k", wk_hbm, w_qkd_ref.at[1]),
        ("d", wd_hbm, w_qkd_ref.at[2]),
        ("offset", decay_offset_hbm, decay_offset_ref),
        ("head_gain", head_gain_hbm, head_gain_ref),
        ("mlp_gain", mlp_gain_hbm, mlp_gain_ref),
        ("v", wv_hbm, wv_ref),
        ("g", wg_hbm, wg_ref),
        ("state", state_hbm, state_ref),
        ("up", w_up_hbm, w_up_ref),
        ("down", w_down_hbm, w_down_ref),
        ("out", w_out_hbm, w_out_ref),
    ):
        group = "q" if name in ("k", "d") else name
        sem = load_sem.at[at_sem.setdefault(group, len(at_sem))]
        loads[name] = pltpu.make_async_copy(source, target, sem)
        if name != "out":
            loads[name].start()
    loads["q"] = pltpu.make_async_copy(w_qkd_ref, w_qkd_ref, load_sem.at[at_sem["q"]])

    @pl.when(tp == 0)
    def _():
        pl.semaphore_wait(barrier, 1)
        signal(ready_sem, kv, 1)

    @pl.when(tp == 1)
    def _():
        loads["out"].start()
        pl.semaphore_wait(ready_sem, 1)

    loads["tokens"].wait()
    tok_copy = remote(tok_ref, tok_all.at[tp], tok_sem.at[0], tok_sem.at[1], kv, other)
    tok_copy.start()

    w_out_copy = remote(w_out_hbm, w_out_other, w_out_sem.at[0], w_out_sem.at[0], kv, 1)
    w_up_copy = remote(w_up_hbm, w_up_other, w_out_sem.at[1], w_out_sem.at[1], kv, 1)
    w_down_copy = remote(
        w_down_hbm.at[:, pl.ds(0, 2 * half)], w_down_other, w_out_sem.at[2], w_out_sem.at[2], kv, 1
    )

    qkd_copies = [
        remote(source, w_qkd_other.at[i], w_out_sem.at[1], w_out_sem.at[1], kv, 1)
        for i, source in enumerate((wq_hbm, wk_hbm, wd_hbm))
    ]
    qkd_all = remote(w_qkd_other, w_qkd_other, w_out_sem.at[1], w_out_sem.at[1], kv, 1)
    upper = kv * 2 >= n_kv
    takes_over = (tp == 1) & (kv == 0)
    hands_over = (tp == 0) & (kv == 0)

    @pl.when(hands_over)
    def _():
        for copy in qkd_copies:
            copy.start()

    @pl.when(tp == 0)
    def _():
        w_out_copy.start()

    @pl.when((tp == 0) & (kv > 0))
    def _():
        w_up_copy.start()


    def group_is_here():
        pl.semaphore_wait(barrier, 2 * (n_kv - 1))
        signal(ready_sem, kv, 0)

    @pl.when((tp == 1) & upper)
    def _():
        group_is_here()

    tok_all[tp] = tok_ref[...]
    tok_own = tok_ref[...].astype(f32)
    squares = jnp.sum(tok_own * tok_own, axis=1, keepdims=True)
    loads["mix_gain"].wait()

    def half_rows(which):
        return pl.ds(pl.multiple_of(which * half, half), half)

    scaled_own = (tok_own * mix_gain_ref[tp]).astype(bf16)
    loads["q"].wait()
    early = [
        jnp.dot(scaled_own, w_qkd_ref[i, half_rows(tp), :], preferred_element_type=f32) for i in range(3)
    ]
    tok_copy.wait_recv()
    tok_other = tok_all[other].astype(f32)
    squares = squares + jnp.sum(tok_other * tok_other, axis=1, keepdims=True)
    scaled_other = (tok_other * mix_gain_ref[other]).astype(bf16)

    groups = ((send_a, recv_a), (send_b, recv_b), (send_c, recv_c))

    def fill(send, total, at):
        columns = total.shape[1]
        for owner in range(n_kv):
            send[owner, :, at : at + columns] = total[owner * seqs : (owner + 1) * seqs].astype(bf16)

    def project(weight_ref):
        total = jnp.dot(scaled_own, weight_ref[half_rows(tp), :], preferred_element_type=f32)
        return total + jnp.dot(scaled_other, weight_ref[half_rows(other), :], preferred_element_type=f32)

    def proj_copy(group, j):
        send, recv = groups[group]
        return remote(send.at[j], recv.at[kv], proj_sem.at[group, 0], proj_sem.at[group, 1], j, tp)

    def proj_all(group):
        send, recv = groups[group]
        some = pl.ds(0, n_kv - 1)
        return remote(send.at[some], recv.at[some], proj_sem.at[group, 0], proj_sem.at[group, 1], kv, other)

    def send_early(group):
        for j in far:

            now = upper & (j != kv - 1)
            if group > 0 and j is not far[0]:
                now = now & (j > kv)

            @pl.when(now)
            def _():
                proj_copy(group, j).start()

    def send_late():
        order = sorted(
            ((group, at) for group in range(3) for at in range(n_kv - 1)),
            key=lambda item: item[1] * 2 + (0 if item[0] == 0 else 3),
        )
        for group, at in order:
            sends = jnp.logical_not(upper)
            if group == 0:
                sends = sends & jnp.logical_not(hands_over)

            @pl.when(sends)
            def _():
                proj_copy(group, far[at]).start()

    wide = jnp.broadcast_to(squares, (rows, 128))
    lane = lax.broadcasted_iota(jnp.int32, (seqs, 128), 1)
    for owner in range(n_kv):
        mine = slice(owner * seqs, (owner + 1) * seqs)
        high = wide[mine].astype(bf16).astype(f32)
        sums = jnp.where(lane < 64, high, wide[mine] - high)
        send_a[owner, :, 3 * key_width :] = sums.astype(bf16)
    late = [
        jnp.dot(scaled_other, w_qkd_ref[i, half_rows(other), :], preferred_element_type=f32) for i in range(3)
    ]
    for i in range(3):
        fill(send_a, early[i] + late[i], i * key_width)

    @pl.when((tp == 0) & upper)
    def _():
        pl.semaphore_wait(ready_sem, 1)

    send_early(0)
    loads["v"].wait()
    loads["g"].wait()
    total_v, total_g = project(wv_ref), project(wg_ref)
    fill(send_b, total_v, 0)
    fill(send_c, total_g, 0)
    send_early(1)
    send_early(2)

    for j in far[1:]:
        for group in (1, 2):

            @pl.when(upper & (j < kv - 1))
            def _():
                proj_copy(group, j).start()

    @pl.when(upper)
    def _():
        for group in range(3):
            proj_copy(group, kv - 1).start()

    def other_copy(j):
        return remote(send_other.at[j], recv_a.at[0], w_out_sem.at[2], proj_sem.at[0, 1], j, 0)

    @pl.when(takes_over)
    def _():
        qkd_all.wait_recv()
        for owner in range(n_kv):
            send_other[owner, :, 3 * key_width :] = send_a[owner, :, 3 * key_width :]
        total = [
            jnp.dot(scaled_own, w_qkd_other[i, half_rows(tp), :], preferred_element_type=f32)
            + jnp.dot(scaled_other, w_qkd_other[i, half_rows(other), :], preferred_element_type=f32)
            for i in range(3)
        ]
        for i in range(3):
            fill(send_other, total[i], i * key_width)

    @pl.when((tp == 1) & jnp.logical_not(upper))
    def _():
        group_is_here()

    @pl.when(takes_over)
    def _():
        for j in range(n_kv - 1, 0, -1):
            other_copy(j).start()


    @pl.when((tp == 0) & jnp.logical_not(upper))
    def _():
        pl.semaphore_wait(ready_sem, 1)

    send_late()

    def gathered(group):
        send, recv = groups[group]
        total = send[kv].astype(f32)
        proj_all(group).wait_recv()
        for j in near:
            total = total + recv[j].astype(f32)
        return total

    group_a = gathered(0)
    row_sums = group_a[:, 3 * key_width : 3 * key_width + 1] + group_a[:, 3 * key_width + 64 : 3 * key_width + 65]
    row_scale = lax.rsqrt(row_sums * (1.0 / width) + epsilon)
    queries = group_a[:, :key_width] * (row_scale * key_dim**-0.5)
    new_keys = group_a[:, key_width : 2 * key_width] * row_scale
    loads["offset"].wait()
    retain = jax.nn.sigmoid(
        group_a[:, 2 * key_width : 3 * key_width] * row_scale + decay_offset_ref[...]
    )
    query_retain = queries * retain
    for h in range(heads):
        coef[h * seqs : (h + 1) * seqs, :] = query_retain[:, h * key_dim : (h + 1) * key_dim]
    queries_t[...] = coef[...].T
    loads["state"].wait()
    for h in range(heads):
        for b in range(seqs):
            at = h * seqs + b
            total = jnp.zeros((8, val_dim), f32)
            for start in range(0, key_dim, ROW_CHUNK):
                piece = slice(start, start + ROW_CHUNK)
                product = queries_t[piece, at : at + 1] * state_ref[b, h, piece, :]
                total = total + jnp.sum(product.reshape(ROW_CHUNK // 8, 8, val_dim), axis=0)
            read[h, b : b + 1, :] = jnp.sum(total, axis=0, keepdims=True)

    overlap = queries * new_keys
    all_dots = [
        jnp.sum(overlap[:, h * key_dim : (h + 1) * key_dim], axis=1, keepdims=True) for h in range(heads)
    ]
    values = gathered(1) * row_scale
    vals[...] = values
    loads["head_gain"].wait()
    normal = []
    for h in range(heads):
        cols = slice(h * val_dim, (h + 1) * val_dim)
        readout = read[h] + all_dots[h] * values[:, cols]
        mean = jnp.mean(readout * readout, axis=1, keepdims=True)
        normal.append(readout * lax.rsqrt(mean + epsilon) * head_gain_ref[...])
    gates = gathered(2) * row_scale
    for h in range(heads):
        cols = slice(h * val_dim, (h + 1) * val_dim)
        gate = gates[:, cols]
        gated_all[tp, kv, :, cols] = (normal[h] * (gate * jax.nn.sigmoid(gate))).astype(bf16)

    def gated_copy(j):
        block = gated_all.at[tp, kv]
        return remote(block, block, gated_sem.at[0], gated_sem.at[1 + tp], j, 1)

    def gated_some(from_tp, count):
        blocks = gated_all.at[from_tp, pl.ds(0, count)]
        return remote(blocks, blocks, gated_sem.at[0], gated_sem.at[1 + from_tp], kv, other)

    for j in far:
        gated_copy(j).start()

    @pl.when(tp == 0)
    def _():
        gated_copy(kv).start()

    @pl.when((tp == 0) & (kv > 0))
    def _():
        w_down_copy.start()

    for h in range(heads):
        cols = slice(h * key_dim, (h + 1) * key_dim)
        update[2 * h * seqs : (2 * h + 1) * seqs, :] = new_keys[:, cols]
        update[(2 * h + 1) * seqs : (2 * h + 2) * seqs, :] = retain[:, cols]
    coef_t[...] = update[...].T
    for h in range(heads):
        for b in range(seqs):
            at = 2 * h * seqs + b
            value_row = vals[b : b + 1, h * val_dim : (h + 1) * val_dim]
            for start in range(0, key_dim, ROW_CHUNK):
                piece = slice(start, start + ROW_CHUNK)
                state_ref[b, h, piece, :] = (
                    coef_t[piece, at + seqs : at + seqs + 1] * state_ref[b, h, piece, :]
                    + coef_t[piece, at : at + 1] * value_row
                )

    tok_copy.wait_send()

    @pl.when(jnp.logical_not(hands_over))
    def _():
        proj_all(0).wait_send()

    for group in (1, 2):
        proj_all(group).wait_send()

    @pl.when(takes_over)
    def _():
        some = send_other.at[pl.ds(0, n_kv - 1)]
        remote(some, some, w_out_sem.at[2], w_out_sem.at[2], kv, 0).wait_send()

    @pl.when(hands_over)
    def _():
        qkd_all.wait_send()

    def stream_copy(j, to_tp, owner):
        block = stream_all.at[owner]
        return remote(block, block, stream_send_sem.at[to_tp], stream_recv_sem.at[owner], j, to_tp)

    def out_rows(from_tp):
        for owner in range(n_kv):
            gated_rows[owner * seqs : (owner + 1) * seqs, :] = gated_all[from_tp, owner].astype(f32)
        return gated_rows[...].astype(bf16)

    @pl.when(tp == 1)
    def _():
        gated_some(1, n_kv - 1).wait_recv()
        loads["out"].wait()
        branch = jnp.dot(out_rows(1), w_out_ref[...], preferred_element_type=f32)
        w_out_copy.wait_recv()
        gated_some(0, n_kv).wait_recv()
        branch = branch + jnp.dot(out_rows(0), w_out_other[...], preferred_element_type=f32)
        for i in range(2):
            stream_all[kv, i] = (tok_all[i].astype(f32) + branch[:, i * half : (i + 1) * half]).astype(bf16)
        for to_tp in (1, 0):
            for j in far:
                stream_copy(j, to_tp, kv).start()
        stream_copy(kv, 0, kv).start()

        gated_some(1, n_kv - 1).wait_send()

    loads["mlp_gain"].wait()
    loads["up"].wait()

    @pl.when(tp == 0)
    def _():
        gated_some(0, n_kv).wait_send()
        w_out_copy.wait_send()

        @pl.when(kv > 0)
        def _():
            w_up_copy.wait_send()
            w_down_copy.wait_send()

        stream_copy(kv, 0, kv).wait_recv()

    def hidden_units(weights_of, waits):
        hidden = [None] * len(weights_of)
        sums = None
        for step, owner in enumerate([kv] + near):
            for wait in waits[step]:
                wait()
            if step > 0:
                stream_copy(kv, tp, owner).wait_recv()
            pieces = [stream_all[owner, i].astype(f32) for i in range(2)]
            normed = jnp.concatenate(
                [(piece * mlp_gain_ref[owner, i]).astype(bf16) for i, piece in enumerate(pieces)], axis=1
            )
            first = pl.multiple_of(owner * (2 * half), 2 * half)
            for at, ref in enumerate(weights_of):
                term = jnp.dot(normed, ref[pl.ds(first, 2 * half), :], preferred_element_type=f32)
                hidden[at] = term if step == 0 else hidden[at] + term
            part = sum(jnp.sum(piece * piece, axis=1, keepdims=True) for piece in pieces)
            sums = part if sums is None else sums + part
        mlp_scale = lax.rsqrt(sums * (1.0 / width) + epsilon)
        active = [jnp.maximum(units * mlp_scale, 0.0) for units in hidden]
        squared = [(units * units).astype(bf16) for units in active]
        squared_ref[...] = squared[0]
        return squared

    serves = (tp == 1) & (kv > 0)

    def down_copy(at, j, to_tp):
        return remote(down_send.at[at, to_tp], down_recv.at[2 * kv + tp], down_sem.at[0], down_sem.at[1], j, to_tp)

    def down_columns(first, columns):
        return jnp.dot(
            squared_ref[...],
            w_down_ref[:, pl.ds(pl.multiple_of(first, half), columns)],
            preferred_element_type=f32,
        )

    def down_chip(at, j):
        term = down_columns(2 * j * half, 2 * half)
        for i in range(2):
            down_send[at, i] = term[:, i * half : (i + 1) * half].astype(bf16)
            down_copy(at, j, i).start()

    def down_pair():
        term = down_columns(2 * kv * half, 2 * half)
        for i in range(2):
            down_own[i] = term[:, i * half : (i + 1) * half]
            down_send[n_kv - 1, i] = term[:, i * half : (i + 1) * half].astype(bf16)
        down_copy(n_kv - 1, kv, other).start()

    @pl.when(serves)
    def _():
        waits = [[w_up_copy.wait_recv], [loads["down"].wait, w_down_copy.wait_recv]] + [[]] * (n_kv - 2)
        squared = hidden_units((w_up_ref, w_up_other), waits)
        for i in range(2):
            cols = slice(i * half, (i + 1) * half)
            term = jnp.dot(squared[0], w_down_ref[:, cols], preferred_element_type=f32)
            term = term + jnp.dot(squared[1], w_down_other[:, cols], preferred_element_type=f32)
            down_send[0, i] = term.astype(bf16)
            down_copy(0, 0, i).start()

    @pl.when(jnp.logical_not(serves))
    def _():
        hidden_units((w_up_ref,), [[], [loads["down"].wait]] + [[]] * (n_kv - 2))

    @pl.when(kv == 0)
    def _():
        down_pair()
        for j in range(n_kv - 1, 0, -1):
            down_chip(j - 1, j)

    @pl.when(kv > 0)
    def _():
        orders = [
            sorted((j for j in range(1, n_kv) if j != me), key=lambda j: (-abs(j - me), j)) for me in range(n_kv)
        ]
        for at in range(n_kv - 2):
            down_chip(at + 1, pick(kv, [order[at] for order in orders]))
        down_pair()


    @pl.when(tp == 1)
    def _():
        remote(stream_all, stream_all, stream_send_sem.at[0], stream_recv_sem.at[0], kv, 0).wait_send()
        some = stream_all.at[pl.ds(0, n_kv - 1)]
        remote(some, some, stream_send_sem.at[1], stream_recv_sem.at[0], kv, 0).wait_send()

    def down_blocks(count):
        some = down_recv.at[pl.ds(0, count)]
        return remote(some, some, down_sem.at[0], down_sem.at[1], kv, other)

    def finish(count, slots):
        total = stream_all[kv, tp].astype(f32) + down_own[tp]
        down_blocks(count).wait_recv()
        for slot in slots:
            total = total + down_recv[slot].astype(f32)
        mixed_ref[...] = total.astype(bf16)

    @pl.when(kv == 0)
    def _():
        finish(n_kv, [other] + [2 * j + 1 for j in range(1, n_kv)])

    @pl.when(kv > 0)
    def _():
        finish(2 * n_kv - 1, [2 * kv + other] + [2 * j + i for j in near for i in range(2)])

    @pl.when((kv == 0) | (tp == 1))
    def _():
        down_blocks(2 * n_kv - 1).wait_send()

    @pl.when((kv > 0) & (tp == 0))
    def _():
        down_blocks(2 * n_kv - 3).wait_send()


def write_kernel(mixed_ref, state_ref, mixed_hbm, state_hbm, state_sem, mixed_sem):
    seqs, heads = state_ref.shape[:2]
    copies = [pltpu.make_async_copy(mixed_ref, mixed_hbm, mixed_sem.at[0])]
    for b in range(seqs):
        for h in range(heads):
            copies.append(
                pltpu.make_async_copy(state_ref.at[b, h], state_hbm.at[b, h], state_sem.at[b, h])
            )
    for copy in copies:
        copy.start()
    for copy in copies:
        copy.wait()


def kernel_shards(
    n_kv,
    tokens,
    state,
    mix_gain,
    w_query,
    w_key,
    w_decay,
    w_value,
    w_gate,
    decay_offset,
    head_gain,
    w_out,
    mlp_gain,
    w_up,
    w_down,
):
    f32, bf16 = jnp.float32, jnp.bfloat16
    rows, half = tokens.shape
    seqs, heads, key_dim, val_dim = state.shape
    key_width, val_width = heads * key_dim, heads * val_dim
    vmem = pl.BlockSpec(memory_space=pltpu.VMEM)
    hbm = pl.BlockSpec(memory_space=pltpu.HBM)
    weights = (w_query, w_key, w_decay, w_value, w_gate, w_out, w_up, w_down)
    a_width = 3 * key_width + 128
    dma = pltpu.SemaphoreType.DMA
    scratch = (
        [
            pltpu.VMEM(tokens.shape, bf16),
            pltpu.VMEM((2, 1, half), f32),
            pltpu.VMEM((1, key_width), f32),
            pltpu.VMEM((1, val_dim), f32),
            pltpu.VMEM((n_kv, 2, 1, half), f32),
        ]
        + [pltpu.VMEM((3,) + w_query.shape, bf16)]
        + [pltpu.VMEM(weight.shape, bf16) for weight in weights[3:]]
        + [
            pltpu.VMEM((3,) + w_query.shape, bf16),
            pltpu.VMEM((n_kv, seqs, a_width), bf16),
            pltpu.VMEM(w_out.shape, bf16),
            pltpu.VMEM(w_up.shape, bf16),
            pltpu.VMEM((w_down.shape[0], 2 * half), bf16),
            pltpu.VMEM((2, rows, half), bf16),
            pltpu.VMEM((n_kv, seqs, a_width), bf16),
            pltpu.VMEM((n_kv, seqs, val_width), bf16),
            pltpu.VMEM((n_kv, seqs, val_width), bf16),
            pltpu.VMEM((n_kv, seqs, a_width), bf16),
            pltpu.VMEM((n_kv, seqs, val_width), bf16),
            pltpu.VMEM((n_kv, seqs, val_width), bf16),
            pltpu.VMEM((heads * seqs, key_dim), f32),
            pltpu.VMEM((key_dim, heads * seqs), f32),
            pltpu.VMEM((2 * heads * seqs, key_dim), f32),
            pltpu.VMEM((key_dim, 2 * heads * seqs), f32),
            pltpu.VMEM((seqs, val_width), f32),
            pltpu.VMEM((heads, seqs, val_dim), f32),
            pltpu.VMEM((2, n_kv, seqs, val_width), bf16),
            pltpu.VMEM((rows, val_width), f32),
            pltpu.VMEM((n_kv, 2, rows, half), bf16),
            pltpu.VMEM((rows, w_up.shape[1]), bf16),
            pltpu.VMEM((n_kv, 2, rows, half), bf16),
            pltpu.VMEM((2, rows, half), f32),
            pltpu.VMEM((2 * n_kv, rows, half), bf16),
            dma((12,)),
            pltpu.SemaphoreType.REGULAR,
            dma((2,)),
            dma((3,)),
            dma((3, 2)),
            dma((3,)),
            dma((2,)),
            dma((n_kv,)),
            dma((2,)),
        ]
    )
    mixed, new_state = pl.pallas_call(
        functools.partial(layer_kernel, n_kv),
        out_shape=(
            pltpu.VMEM(tokens.shape, bf16),
            pltpu.VMEM(state.shape, f32),
        ),
        in_specs=[hbm] * 14,
        out_specs=(vmem, vmem),
        scratch_shapes=scratch,
        compiler_params=pltpu.CompilerParams(
            collective_id=0, has_side_effects=True, vmem_limit_bytes=VMEM_BYTES - 4 * state.size - 2**19
        ),
    )(
        tokens,
        mix_gain.reshape(2, 1, half),
        decay_offset.reshape(1, key_width),
        head_gain.reshape(1, val_dim),
        mlp_gain.reshape(n_kv, 2, 1, half),
        state,
        *weights,
    )
    return pl.pallas_call(
        write_kernel,
        out_shape=(
            jax.ShapeDtypeStruct(tokens.shape, bf16),
            jax.ShapeDtypeStruct(state.shape, f32),
        ),
        in_specs=[vmem] * 2,
        out_specs=(hbm, hbm),
        scratch_shapes=[dma((seqs, heads)), dma((1,))],
        compiler_params=pltpu.CompilerParams(vmem_limit_bytes=2**20),
    )(
        pltpu.with_memory_space_constraint(mixed, pltpu.VMEM),
        pltpu.with_memory_space_constraint(new_state, pltpu.VMEM),
    )


def fits_kernel(mesh):
    n_kv, n_tp = mesh.shape["kv"], mesh.shape["tp"]
    return n_tp == 2 and n_kv > 1 and D % (128 * n_kv * n_tp) == 0


def solution(mesh):
    in_specs = (
        P("dp", ("kv", "tp")),
        P(("dp", "kv"), "tp", None, None),
        P("kv"),
        P("kv", "tp"),
        P("kv", "tp"),
        P("kv", "tp"),
        P("kv", "tp"),
        P("kv", "tp"),
        P("tp"),
        P(),
        P("tp", "kv"),
        P(),
        P(None, ("kv", "tp")),
        P(("kv", "tp"), None),
    )
    out_specs = (P("dp", ("kv", "tp")), P(("dp", "kv"), "tp", None, None))
    shards = plain_shards
    if fits_kernel(mesh):
        shards = functools.partial(kernel_shards, mesh.shape["kv"])
    return jax.shard_map(shards, mesh=mesh, in_specs=in_specs, out_specs=out_specs, check_vma=False)
```
